32 devices in a mesh: sp: 32 (over z, y, x, core), tp: 1.
Axes of the slice: x: 2, y: 2, z: 4, core: 2. Of those that a mesh axis runs over, the one named last changes fastest.
Arguments:
- queries: bfloat16 [4096, 2048], P('sp', 'tp'), may hold values from -6 to 6
- forget_logits: bfloat16 [2, 4096, 2048], P(None, 'sp', 'tp'), may hold values from -7.5 to 7.5
- value_matrix: bfloat16 [4096, 2048], P('sp', 'tp'), may hold values from -6 to 6
- output_gate_logits: bfloat16 [4096, 2048], P('sp', 'tp'), may hold values from -6 to 6
- forget_slack: float32 [2048], P('tp'), may hold values from 0.00012207031 to 0.07
- spike_log_forget: float32 [4096, 16], P('sp', 'tp'), may hold values from -2.8 to 0, as said below
- head_norm_gain: bfloat16 [128], replicated, may hold values from 0.099609375 to 1.8984375
- output_weight: bfloat16 [2048, 2048], P('tp'), may hold values from -0.125 to 0.125
- residual: bfloat16 [4096, 2048], P('sp'), may hold values from -6 to 6
- mixer_norm_gain: bfloat16 [2048], replicated, may hold values from 0.099609375 to 1.8984375
- mixer_gate_weight: bfloat16 [2048, 5632], P('sp', 'tp'), may hold values from -0.125 to 0.125
- mixer_up_weight: bfloat16 [2048, 5632], P('sp', 'tp'), may hold values from -0.125 to 0.125
- mixer_down_weight: bfloat16 [5632, 2048], P('tp', 'sp'), may hold values from -0.078125 to 0.078125
Outputs:
- layer_out: bfloat16 [4096, 2048], P(('sp', 'tp'))
The draws below stay inside these ranges and needn't reach their ends.
Inputs may be any that keep to these rules, and one draw needn't show every extreme that they name: `spike_log_forget`: zero at all but a few tokens.
All inputs are finite; a program needn't handle non-finite values.
Results may differ from the reference program's by a relative error of at most 0.015.
Values may be sent and summed in bfloat16 or wider, within the bound.
A program may use at most 192 MiB of HBM per device.

```python
import jax
import jax.numpy as jnp
from jax import lax

D = 2048
FF = 5632
HEADS = 16
HEAD = 128
BLOCK = 128
TOK_DEV = 128
TOKENS = 4096
N_TP = 1


def quick_heads(key, quick_count):
    pick_key = jax.random.fold_in(jax.random.fold_in(key, 23), 0)
    ordering = jax.random.permutation(pick_key, HEADS)
    return ordering < quick_count


def draw_forget_logits(key, part):
    noise_key, steady_key, slow_key, channel_key = jax.random.split(jax.random.fold_in(key, 11), 4)
    channels = HEADS * HEAD
    blocks_count = TOKENS // TOK_DEV
    quick_count = HEADS // 2
    slow_share = 0.5
    quick = quick_heads(key, quick_count)
    slow_block = jax.random.uniform(slow_key, (2, blocks_count, HEADS), jnp.float32) < slow_share
    quick_shift = jnp.where(slow_block, 6.0, -3.0)
    steady_shift = jax.random.uniform(steady_key, (2, blocks_count, HEADS), jnp.float32, -6.0, 1.5)
    head_shift = jnp.where(quick[None, None, :], quick_shift, steady_shift)
    channel_shift = jax.random.uniform(channel_key, (2, blocks_count, HEADS, HEAD), jnp.float32, -1.0, 1.0)
    shifted = (head_shift[:, :, :, None] + channel_shift).reshape(2, blocks_count, 1, channels)
    noise = jnp.clip(jax.random.normal(noise_key, (2, blocks_count, TOK_DEV, channels), jnp.float32), -6.0, 6.0)
    total = jnp.clip(shifted + noise, -7.5, 7.5)
    return total.reshape(2, TOKENS, channels).astype(jnp.bfloat16)


def draw_forget_slack(key, part):
    fast_key = jax.random.fold_in(jax.random.fold_in(key, 23), 1)
    slow_key = jax.random.fold_in(jax.random.fold_in(key, 23), 2)
    quick_count = HEADS // 2
    quick = quick_heads(key, quick_count)[:, None]
    quick_rate = jnp.exp(jax.random.uniform(fast_key, (HEADS, HEAD), jnp.float32, jnp.log(0.02), jnp.log(0.07)))
    steady_rate = jnp.exp(jax.random.uniform(slow_key, (HEADS, HEAD), jnp.float32, jnp.log(0.5), jnp.log(2.0))) / TOKENS
    return jnp.where(quick, quick_rate, steady_rate).reshape(HEADS * HEAD)


def draw_spike_log_forget(key, part):
    place_key, depth_key = jax.random.split(jax.random.fold_in(key, 37))
    spots = jax.random.randint(place_key, (4,), 0, TOKENS)
    upper = jnp.log(0.8)
    depths = jax.random.uniform(depth_key, (4, HEADS), jnp.float32, jnp.log(0.5), upper)
    hits = (jnp.arange(TOKENS)[:, None] == spots[None, :]).astype(jnp.float32)
    return jnp.dot(hits, depths)


def block_levels(stream_key, dims, pieces, least, top_value):
    def one(axis_at, parts):
        heights = jax.random.uniform(jax.random.fold_in(jax.random.fold_in(stream_key, 6), axis_at), (parts,), jnp.float32, least / len(pieces), top_value / len(pieces))
        return jnp.repeat(jnp.exp(heights), dims[axis_at] // parts).reshape((-1,) + (1,) * (len(dims) - axis_at - 1))

    gain = one(*pieces[0])
    for cut in pieces[1:]:
        gain = gain * one(*cut)
    return gain


def scatter_about(own_key, dims, spread, most, pieces=(), held_as=jnp.bfloat16):
    values = spread * jax.random.normal(own_key, dims, jnp.float32)
    if pieces:
        values = values * block_levels(own_key, dims, pieces, -0.22, 0.18)
    return jnp.clip(values, -most, most).astype(held_as)


def setup_inputs(seed: int = 0) -> dict:
    seeds = jax.random.split(jax.random.key(seed), 14)
    queries = scatter_about(seeds[0], (TOKENS, HEADS * HEAD), 1.0, 6.0, ((0, 32),))
    forget_logits = draw_forget_logits(jax.random.fold_in(seeds[13], 71), 0)
    value_matrix = scatter_about(seeds[2], (TOKENS, HEADS * HEAD), 1.0, 6.0, ((0, 32),))
    output_gate_logits = scatter_about(seeds[3], (TOKENS, HEADS * HEAD), 1.0, 6.0, ((0, 32),))
    forget_slack = draw_forget_slack(jax.random.fold_in(seeds[13], 71), 0)
    spike_log_forget = draw_spike_log_forget(jax.random.fold_in(seeds[13], 71), 0)
    head_norm_gain = jnp.clip(1.0 + 0.18 * jax.random.normal(seeds[6], (HEAD,), jnp.float32), 0.099609375, 1.8984375).astype(jnp.bfloat16)
    output_weight = scatter_about(seeds[7], (HEADS * HEAD, D), (HEADS * HEAD) ** -0.5, 0.125)
    residual = scatter_about(seeds[8], (TOKENS, D), 1.0, 6.0, ((0, 32),))
    mixer_norm_gain = jnp.clip(1.0 + 0.18 * jax.random.normal(seeds[9], (D,), jnp.float32), 0.099609375, 1.8984375).astype(jnp.bfloat16)
    mixer_gate_weight = scatter_about(seeds[10], (D, FF), D ** -0.5, 0.125, ((0, 32),))
    mixer_up_weight = scatter_about(seeds[11], (D, FF), D ** -0.5, 0.125, ((0, 32),))
    mixer_down_weight = scatter_about(seeds[12], (FF, D), FF ** -0.5, 0.078125, ((1, 32),))
    return dict(queries=queries, forget_logits=forget_logits, value_matrix=value_matrix, output_gate_logits=output_gate_logits, forget_slack=forget_slack, spike_log_forget=spike_log_forget, head_norm_gain=head_norm_gain, output_weight=output_weight, residual=residual, mixer_norm_gain=mixer_norm_gain, mixer_gate_weight=mixer_gate_weight, mixer_up_weight=mixer_up_weight, mixer_down_weight=mixer_down_weight)


NORM_EPS = 1e-06
BEST_PRECISION = lax.Precision.HIGHEST

def rms_scale(entries, gain_vec):
    return entries * lax.rsqrt(lax.optimization_barrier(jnp.mean(entries * entries, axis=-1, keepdims=True)) + NORM_EPS) * gain_vec.astype(jnp.float32)

def full_sweep(query_f, key_f, decay_f, value_f):
    total_rows, heads_all, head_width = query_f.shape
    blocks_count = total_rows // BLOCK
    tri_mask = jnp.tril(jnp.ones((BLOCK, BLOCK), bool))

    def to_blocks(tensor):
        return tensor.reshape(blocks_count, BLOCK, heads_all, head_width)

    def advance(state_now, segment):
        query_seg, key_seg, decay_seg, value_seg = segment
        running = jnp.cumsum(decay_seg, axis=0)
        query_scaled = query_seg * jnp.exp(running)
        key_scaled = key_seg * jnp.exp(-running)
        scores = jnp.einsum('thd,shd->hts', query_scaled, key_scaled, precision=BEST_PRECISION)
        scores = jnp.where(tri_mask[None], scores, 0.0)
        result = jnp.einsum('hts,shv->thv', scores, value_seg, precision=BEST_PRECISION)
        result = result + jnp.einsum('thd,hdv->thv', query_scaled, state_now, precision=BEST_PRECISION)
        final_log = running[-1]
        state_next = jnp.exp(final_log)[:, :, None] * state_now + jnp.einsum('shd,shv->hdv', key_seg * jnp.exp(final_log[None] - running), value_seg, precision=BEST_PRECISION)
        return (state_next, result)
    initial = jnp.zeros((heads_all, head_width, head_width), jnp.float32)
    _, results = lax.scan(advance, initial, (to_blocks(query_f), to_blocks(key_f), to_blocks(decay_f), to_blocks(value_f)))
    return results.reshape(total_rows, heads_all, head_width)

def reference(queries, forget_logits, value_matrix, output_gate_logits, forget_slack, spike_log_forget, head_norm_gain, output_weight, residual, mixer_norm_gain, mixer_gate_weight, mixer_up_weight, mixer_down_weight):
    total_rows = queries.shape[0]
    query_f = (jax.nn.silu(queries.astype(jnp.float32)) * HEAD ** (-0.5)).reshape(total_rows, HEADS, HEAD)
    value_f = value_matrix.astype(jnp.float32).reshape(total_rows, HEADS, HEAD)
    gate_random_key = (forget_slack * jax.nn.sigmoid(-forget_logits.astype(jnp.float32))).reshape(2, total_rows, HEADS, HEAD)
    decay_logarithm = jnp.log1p(-gate_random_key) + spike_log_forget[None, :, :, None]
    forward_out = full_sweep(query_f, gate_random_key[0], decay_logarithm[0], value_f)
    backward_out = jnp.flip(full_sweep(jnp.flip(query_f, 0), jnp.flip(gate_random_key[1], 0), jnp.flip(decay_logarithm[1], 0), jnp.flip(value_f, 0)), 0)
    mixture = forward_out + backward_out
    mixed = (rms_scale(mixture, head_norm_gain).reshape(total_rows, HEADS * HEAD) * jax.nn.silu(output_gate_logits.astype(jnp.float32))).astype(jnp.bfloat16)
    group_cols = HEADS * HEAD // N_TP
    summed = residual.astype(jnp.float32)
    for group_index in range(N_TP):
        low_col = group_index * group_cols
        partial_out = jnp.dot(mixed[:, low_col:low_col + group_cols], output_weight[low_col:low_col + group_cols], preferred_element_type=jnp.float32).astype(jnp.bfloat16)
        summed = summed + lax.optimization_barrier(partial_out).astype(jnp.float32)
    hidden_state = summed.astype(jnp.bfloat16)
    unit_cols = FF // N_TP

    def channel_mix(hidden_seg):
        normed = rms_scale(hidden_seg.astype(jnp.float32), mixer_norm_gain).astype(jnp.bfloat16)
        gate_act = jnp.dot(normed, mixer_gate_weight, preferred_element_type=jnp.float32)
        up_act = jnp.dot(normed, mixer_up_weight, preferred_element_type=jnp.float32)
        inner = (jax.nn.silu(gate_act) * up_act).astype(jnp.bfloat16)
        summed_seg = hidden_seg.astype(jnp.float32)
        for group_index in range(N_TP):
            low_unit = group_index * unit_cols
            lowered = jnp.dot(inner[:, low_unit:low_unit + unit_cols], mixer_down_weight[low_unit:low_unit + unit_cols], preferred_element_type=jnp.float32).astype(jnp.bfloat16)
            summed_seg = summed_seg + lax.optimization_barrier(lowered).astype(jnp.float32)
        return summed_seg.astype(jnp.bfloat16)
    hidden_blocks = hidden_state.reshape(total_rows // TOK_DEV, TOK_DEV, D)
    return lax.map(channel_mix, hidden_blocks).reshape(total_rows, D)
```

```python
import functools

import jax
import jax.numpy as jnp
from jax import lax
from jax.experimental import pallas as pl
from jax.experimental.pallas import tpu as pltpu
from jax.sharding import PartitionSpec as P

NORM_EPS = 1e-06
MESH = pl.DeviceIdType.MESH
PAD_ROWS = 16
GROUP = 8


def dot_nt(a, b):
    return lax.dot_general(a, b, (((1,), (1,)), ((), ())), preferred_element_type=jnp.float32)


def dot_tn(a, b):
    return lax.dot_general(a, b, (((0,), (0,)), ((), ())), preferred_element_type=jnp.float32)


def dot_nn(a, b):
    return jnp.dot(a, b, preferred_element_type=jnp.float32)


def silu(x):
    return x * jax.nn.sigmoid(x)


def split_bf16(x):
    high = x.astype(jnp.bfloat16)
    return high, (x - high.astype(jnp.float32)).astype(jnp.bfloat16)


def sweep_kernel(q_ref, f_ref, v_ref, slack_ref, spike_ref, local_ref, reach_ref, state_ref):
    head = pl.program_id(0)
    rows, width = q_ref.shape
    query = silu(q_ref[...].astype(jnp.float32)) * (width ** -0.5)
    value = v_ref[...]
    spikes = spike_ref[...]
    lane = lax.broadcasted_iota(jnp.int32, spikes.shape, 1)
    spike = jnp.sum(jnp.where(lane == head, spikes, 0.0), axis=1, keepdims=True)
    slack = slack_ref[...]
    down = lax.broadcasted_iota(jnp.int32, (rows, rows), 0)
    across = lax.broadcasted_iota(jnp.int32, (rows, rows), 1)
    scores = None
    for way in (0, 1):
        mask = (down >= across) if way == 0 else (down <= across)
        tri = jnp.where(mask, 1.0, 0.0).astype(jnp.bfloat16)
        key = slack * jax.nn.sigmoid(-f_ref[way].astype(jnp.float32))
        decay = jnp.log1p(-key) + spike
        high, low = split_bf16(decay)
        running = dot_nn(tri, high) + dot_nn(tri, low)
        final = running[rows - 1 : rows] if way == 0 else running[0:1]
        query_scaled = (query * jnp.exp(running)).astype(jnp.bfloat16)
        key_scaled = (key * jnp.exp(-running)).astype(jnp.bfloat16)
        key_end = (key * jnp.exp(final - running)).astype(jnp.bfloat16)
        part = jnp.where(mask, dot_nt(query_scaled, key_scaled), 0.0)
        scores = part if scores is None else scores + part
        reach_ref[way] = query_scaled
        state_ref[way, 0, 0:width] = dot_tn(value, key_end).astype(jnp.bfloat16)
        total_high, total_low = split_bf16(jnp.exp(final))
        place = lax.broadcasted_iota(jnp.int32, (PAD_ROWS, width), 0)
        state_ref[way, 0, width : width + PAD_ROWS] = jnp.where(
            place == 0,
            total_high.astype(jnp.float32),
            jnp.where(place == 1, total_low.astype(jnp.float32), 0.0),
        ).astype(jnp.bfloat16)
    local_ref[...] = dot_nn(scores.astype(jnp.bfloat16), value)


def sweep(queries, forget_logits, values, slack, spike):
    rows, columns = queries.shape
    heads = spike.shape[1]
    width = columns // heads
    by_head = pl.BlockSpec((rows, width), lambda h: (0, h))
    return pl.pallas_call(
        sweep_kernel,
        grid=(heads,),
        in_specs=[
            by_head,
            pl.BlockSpec((2, rows, width), lambda h: (0, 0, h)),
            by_head,
            pl.BlockSpec((1, width), lambda h: (0, h)),
            pl.BlockSpec((rows, heads), lambda h: (0, 0)),
        ],
        out_specs=[
            by_head,
            pl.BlockSpec((2, rows, width), lambda h: (0, 0, h)),
            pl.BlockSpec((2, 1, width + PAD_ROWS, width), lambda h: (0, h, 0, 0)),
        ],
        out_shape=[
            jax.ShapeDtypeStruct((rows, columns), jnp.float32),
            jax.ShapeDtypeStruct((2, rows, columns), jnp.bfloat16),
            jax.ShapeDtypeStruct((2, heads, width + PAD_ROWS, width), jnp.bfloat16),
        ],
        cost_estimate=pl.CostEstimate(
            flops=20 * rows * width * columns, bytes_accessed=8 * rows * columns, transcendentals=8 * rows * columns
        ),
        name="sweep",
    )(queries, forget_logits, values, slack.reshape(1, columns), spike)


def greet(axis, others, count):
    barrier = pltpu.get_barrier_semaphore()

    def signal(k, carry):
        pl.semaphore_signal(barrier, inc=1, device_id={axis: others(k)}, device_id_type=MESH)
        return carry

    lax.fori_loop(1, count, signal, 0)
    pl.semaphore_wait(barrier, count - 1)


def exchange_kernel(n, state_ref, enter_ref, held, made, out_sem, in_sem, out_sem2, in_sem2):
    me = lax.axis_index("sp")
    rows = enter_ref.shape[1]

    def other(k):
        return lax.rem(me + k, n)

    greet("sp", other, n)

    def first(k):
        there = other(k)
        return pltpu.make_async_remote_copy(
            src_ref=state_ref.at[there],
            dst_ref=held.at[me],
            send_sem=out_sem.at[k],
            recv_sem=in_sem.at[k],
            device_id={"sp": there},
            device_id_type=MESH,
        )

    def second(k):
        there = other(k)
        return pltpu.make_async_remote_copy(
            src_ref=made.at[there],
            dst_ref=enter_ref.at[me],
            send_sem=out_sem2.at[k],
            recv_sem=in_sem2.at[k],
            device_id={"sp": there},
            device_id_type=MESH,
        )

    def go(copy):
        def start(k, carry):
            copy(k).start()
            return carry

        lax.fori_loop(1, n, start, 0)

    def end(copy):
        def wait(k, carry):
            copy(k).wait()
            return carry

        lax.fori_loop(1, n, wait, 0)

    go(first)
    held[me] = state_ref[me]
    end(first)
    backward = me // (n // 2)

    def step(i, total):
        source = i + backward * (n - 1 - 2 * i)
        made[source] = total.astype(jnp.bfloat16)
        block = held[source].astype(jnp.float32)
        factor = block[rows : rows + 1] + block[rows + 1 : rows + 2]
        return factor * total + block[:rows]

    lax.fori_loop(0, n, step, jnp.zeros(enter_ref.shape[1:], jnp.float32))
    go(second)
    enter_ref[me] = made[me]
    end(second)


def exchange(states):
    n = lax.axis_size("sp")
    ways, heads, padded, width = states.shape
    depth = padded - PAD_ROWS
    cuts = n // (ways * heads)
    rows = depth // cuts
    if cuts > 1:
        body = states[:, :, :depth].reshape(ways, heads, cuts, rows, width)
        tail = jnp.broadcast_to(
            states[:, :, None, depth:], (ways, heads, cuts, PAD_ROWS, width)
        )
        states = jnp.concatenate([body, tail], axis=3)
    entered = pl.pallas_call(
        functools.partial(exchange_kernel, n),
        in_specs=[pl.BlockSpec(memory_space=pltpu.VMEM)],
        out_specs=pl.BlockSpec(memory_space=pltpu.VMEM),
        out_shape=jax.ShapeDtypeStruct((n, rows, width), jnp.bfloat16),
        scratch_shapes=[
            pltpu.VMEM((n, rows + PAD_ROWS, width), jnp.bfloat16),
            pltpu.VMEM((n, rows, width), jnp.bfloat16),
            pltpu.SemaphoreType.DMA((n,)),
            pltpu.SemaphoreType.DMA((n,)),
            pltpu.SemaphoreType.DMA((n,)),
            pltpu.SemaphoreType.DMA((n,)),
        ],
        compiler_params=pltpu.CompilerParams(collective_id=1, has_side_effects=True),
        name="exchange",
    )(states.reshape(n, rows + PAD_ROWS, width))
    return entered.reshape(ways, heads, depth, width)


def reshard_kernel(g, *refs):
    count = (len(refs) - 3) // 2
    gives, takes = refs[:count], refs[count : 2 * count]
    out_sem, in_sem, own_sem = refs[2 * count :]
    me = lax.axis_index("sp")
    base = me // g * g
    seat = me - base

    def other(k):
        return lax.rem(seat + k, g)

    greet("sp", lambda k: base + other(k), g)
    copies = []
    for k in range(1, g):
        there = other(k)
        for i in range(count):
            copies.append(
                pltpu.make_async_remote_copy(
                    src_ref=gives[i].at[there],
                    dst_ref=takes[i].at[seat],
                    send_sem=out_sem.at[i, k],
                    recv_sem=in_sem.at[i, k],
                    device_id={"sp": base + there},
                    device_id_type=MESH,
                )
            )
            copies[-1].start()
    for i in range(count):
        copies.append(pltpu.make_async_copy(gives[i].at[seat], takes[i].at[seat], own_sem.at[i]))
        copies[-1].start()
    for copy in copies:
        copy.wait()


def reshard(arrays, g, collective_id):
    count = len(arrays)
    return pl.pallas_call(
        functools.partial(reshard_kernel, g),
        in_specs=[pl.BlockSpec(memory_space=pltpu.VMEM)] * count,
        out_specs=[pl.BlockSpec(memory_space=pltpu.VMEM)] * count,
        out_shape=[jax.ShapeDtypeStruct(a.shape, a.dtype) for a in arrays],
        scratch_shapes=[
            pltpu.SemaphoreType.DMA((count, g)),
            pltpu.SemaphoreType.DMA((count, g)),
            pltpu.SemaphoreType.DMA((count,)),
        ],
        compiler_params=pltpu.CompilerParams(
            collective_id=collective_id, has_side_effects=True
        ),
        name="reshard",
    )(*arrays)


def gather_kernel(g, give, take, out_sem, in_sem):
    me = lax.axis_index("sp")
    base = me // g * g
    seat = me - base

    def other(k):
        return lax.rem(seat + k, g)

    greet("sp", lambda k: base + other(k), g)
    copies = []
    for k in range(1, g):
        copies.append(
            pltpu.make_async_remote_copy(
                src_ref=give,
                dst_ref=take.at[seat],
                send_sem=out_sem.at[k],
                recv_sem=in_sem.at[k],
                device_id={"sp": base + other(k)},
                device_id_type=MESH,
            )
        )
        copies[-1].start()
    take[seat] = give[...]
    for copy in copies:
        copy.wait()


def gather(array, g, collective_id):
    return pl.pallas_call(
        functools.partial(gather_kernel, g),
        in_specs=[pl.BlockSpec(memory_space=pltpu.VMEM)],
        out_specs=pl.BlockSpec(memory_space=pltpu.VMEM),
        out_shape=jax.ShapeDtypeStruct((g,) + array.shape, array.dtype),
        scratch_shapes=[pltpu.SemaphoreType.DMA((g,)), pltpu.SemaphoreType.DMA((g,))],
        compiler_params=pltpu.CompilerParams(
            collective_id=collective_id, has_side_effects=True
        ),
        name="gather",
    )(array).reshape((g * array.shape[0],) + array.shape[1:])


def project_kernel(local_ref, reach_ref, enter_ref, gain_ref, gate_ref, weight_ref, out_ref, total):
    head = pl.program_id(0)
    mix = (
        local_ref[...]
        + dot_nt(reach_ref[0], enter_ref[0, 0])
        + dot_nt(reach_ref[1], enter_ref[1, 0])
    )
    scale = lax.rsqrt(jnp.mean(mix * mix, axis=-1, keepdims=True) + NORM_EPS)
    gate = silu(gate_ref[...].astype(jnp.float32))
    mixed = (mix * scale * gain_ref[...].astype(jnp.float32) * gate).astype(jnp.bfloat16)
    term = dot_nn(mixed, weight_ref[...])

    @pl.when(head == 0)
    def _():
        total[...] = term

    @pl.when(head > 0)
    def _():
        total[...] += term

    @pl.when(head == pl.num_programs(0) - 1)
    def _():
        out_ref[...] = total[...].astype(jnp.bfloat16)


def project(local, reach, entered, gain, gate_logits, weight):
    rows, columns = local.shape
    heads, width = entered.shape[1], entered.shape[3]
    model = weight.shape[1]
    by_head = pl.BlockSpec((rows, width), lambda h: (0, h))
    return pl.pallas_call(
        project_kernel,
        grid=(heads,),
        in_specs=[
            by_head,
            pl.BlockSpec((2, rows, width), lambda h: (0, 0, h)),
            pl.BlockSpec((2, 1, width, width), lambda h: (0, h, 0, 0)),
            pl.BlockSpec((1, width), lambda h: (0, 0)),
            by_head,
            pl.BlockSpec((width, model), lambda h: (h, 0)),
        ],
        out_specs=pl.BlockSpec((rows, model), lambda h: (0, 0)),
        out_shape=jax.ShapeDtypeStruct((rows, model), jnp.bfloat16),
        scratch_shapes=[pltpu.VMEM((rows, model), jnp.float32)],
        cost_estimate=pl.CostEstimate(
            flops=2 * rows * columns * model, bytes_accessed=2 * columns * model, transcendentals=rows * columns
        ),
        name="project",
    )(local, reach, entered, gain.reshape(1, width), gate_logits, weight)


CORES = 2
PLANE = 4


def flip(i, k):
    out, bit = i, 1
    while bit <= k:
        if k & bit:
            out = out + bit - 2 * bit * (lax.rem(i // bit, 2))
        bit *= 2
    return out


def layer_kernel(
    nz,
    q_hbm, f_hbm, v_hbm, og_hbm, res_hbm, slack_ref, spike_ref, hgain_ref, mgain_ref, wo_hbm, gate_hbm, up_hbm, down_hbm,
    out_ref,
    q_v, f_v, v_v, og_v, res_v, wo_v, w_v,
    reach, scaled, locals_, states, held, total, totals_in, entry, made, enter, mixed, tok, parts, terms,
    in_sem, w0_sem, w1_out, w1_in, x_out, x_in, y_out, y_in, d_out, d_in, p_out, p_in,
    s1_out, s1_in, s2_out, s2_in, s3_out, s3_in, up_out, up_in, dn_out, dn_in, r_out, r_in,
):
    rows, columns = q_v.shape
    width = hgain_ref.shape[1]
    heads = columns // width
    depth = gate_hbm.shape[0]
    units = w_v.shape[2]
    side = PLANE * CORES
    per = 2 * heads // side
    half = side // 2
    me = lax.axis_index("sp")
    z, seat = me // side, lax.rem(me, side)
    q, c = seat // CORES, lax.rem(seat, CORES)
    base = z * side

    def at(zz, qq, cc):
        return zz * side + qq * CORES + cc

    def copy(src, dst, out_sem, got_sem, there):
        return pltpu.make_async_remote_copy(
            src_ref=src, dst_ref=dst, send_sem=out_sem, recv_sem=got_sem,
            device_id={"sp": there}, device_id_type=MESH,
        )

    zs = [z] + [flip(z, k) for k in range(1, nz)]
    qs = [q] + [flip(q, k) for k in range(1, PLANE)]
    along = [at(zz, q, c) for zz in zs]
    x_dev, y_dev, p_dev = at(z, qs[1], c), at(z, qs[2], c), at(z, q, 1 - c)

    loads = [
        pltpu.make_async_copy(src, dst, in_sem.at[i])
        for i, (src, dst) in enumerate(
            ((f_hbm, f_v), (q_hbm, q_v), (v_hbm, v_v), (og_hbm, og_v), (res_hbm, res_v), (wo_hbm, wo_v))
        )
    ]
    weights = (gate_hbm, up_hbm, down_hbm)

    def cut(a, zz):
        return weights[a].at[:, pl.ds(pl.multiple_of(zz * units, 128), units)]

    def piece(zz, qq, cc):
        return w_v.at[:, pl.ds(pl.multiple_of(at(zz, qq, cc) * depth, depth), depth), :]

    def strip(a, device):
        return w_v.at[a, pl.ds(pl.multiple_of(device * depth, depth), depth), :]

    own = [pltpu.make_async_copy(cut(a, z), strip(a, me), w0_sem.at[a]) for a in range(3)]
    for load in loads[:3]:
        load.start()
    for load in own:
        load.start()

    barrier = pltpu.get_barrier_semaphore()
    for k in range(1, nz):
        pl.semaphore_signal(barrier, inc=1, device_id={"sp": along[k]}, device_id_type=MESH)
    for k in range(1, side):
        pl.semaphore_signal(
            barrier, inc=1, device_id={"sp": base + lax.rem(seat + k, side)}, device_id_type=MESH
        )
    pl.semaphore_wait(barrier, nz - 1 + side - 1)

    def first(k):
        return [copy(cut(a, zs[k]), strip(a, me), w1_out.at[a, k], w1_in.at[a, k], along[k]) for a in range(3)]

    def plane(k, sems, there):
        src = piece(zs[k], q, c)
        return copy(src, src, sems[0].at[k], sems[1].at[k], there)

    def corner(k):
        near, there = (1, y_dev) if k < nz // 2 else (2, x_dev)
        src = piece(zs[k], qs[near], c)
        return copy(src, src, d_out.at[k], d_in.at[k], there)

    def partner(k, j):
        src = piece(zs[k], qs[j], c)
        return copy(src, src, p_out.at[k, j], p_in.at[k, j], p_dev)

    def spread(k):
        if k == 0:
            for load in own:
                load.wait()
        else:
            for one in first(k):
                one.wait_recv()
        plane(k, (x_out, x_in), x_dev).start()
        plane(k, (y_out, y_in), y_dev).start()
        partner(k, 0).start()

    def onward(k):
        plane(k, (x_out, x_in), x_dev).wait_recv()
        if k < nz // 2:
            corner(k).start()
        partner(k, 1).start()
        plane(k, (y_out, y_in), y_dev).wait_recv()
        if k >= nz // 2:
            corner(k).start()
        partner(k, 2).start()

    def last(k):
        corner(k).wait_recv()
        partner(k, 3).start()

    late = nz - 1
    for k in range(1, late):
        for one in first(k):
            one.start()
    spread(0)
    for load in loads[3:]:
        load.start()

    down = lax.broadcasted_iota(jnp.int32, (rows, rows), 0)
    across = lax.broadcasted_iota(jnp.int32, (rows, rows), 1)
    masks = (down >= across, down <= across)
    for load in loads[:3]:
        load.wait()
    spikes = spike_ref[...]
    lane = lax.broadcasted_iota(jnp.int32, spikes.shape, 1)
    place = lax.broadcasted_iota(jnp.int32, (PAD_ROWS, width), 0)

    def pad(decay):
        high, low = split_bf16(decay)
        return jnp.where(
            place == 0, high.astype(jnp.float32), jnp.where(place == 1, low.astype(jnp.float32), 0.0)
        ).astype(jnp.bfloat16)

    def by_head(head):
        return pl.ds(pl.multiple_of(head * width, width), width)

    def state_copy(w):
        return copy(states.at[w], held.at[seat], s1_out.at[w], s1_in.at[seat], base + w)

    def state_arrival(w):
        return copy(states.at[w], held.at[w], s1_out.at[w], s1_in.at[w], base + w)

    def make_states(group):
        def step(i, carry):
            head = group * per + i
            lanes = by_head(head)
            query = silu(q_v[:, lanes].astype(jnp.float32)) * (width ** -0.5)
            value = v_v[:, lanes]
            spike = jnp.sum(jnp.where(lane == head, spikes, 0.0), axis=1, keepdims=True)
            slack = slack_ref[:, lanes]
            for way in (0, 1):
                tri = jnp.where(masks[way], 1.0, 0.0).astype(jnp.bfloat16)
                key = slack * jax.nn.sigmoid(-f_v[way, :, lanes].astype(jnp.float32))
                decay = jnp.log1p(-key) + spike
                high, low = split_bf16(decay)
                running = dot_nn(tri, high) + dot_nn(tri, low)
                final = running[rows - 1 : rows] if way == 0 else running[0:1]
                reach[way, :, lanes] = (query * jnp.exp(running)).astype(jnp.bfloat16)
                scaled[way, :, lanes] = (key * jnp.exp(-running)).astype(jnp.bfloat16)
                key_end = (key * jnp.exp(final - running)).astype(jnp.bfloat16)
                states[way * half + group, i, 0:width] = dot_tn(value, key_end).astype(jnp.bfloat16)
                states[way * half + group, i, width : width + PAD_ROWS] = pad(jnp.exp(final))
            return carry

        lax.fori_loop(0, per, step, 0)

    for group in range(half):
        make_states(group)
        for w in (group, half + group):
            @pl.when(w != seat)
            def _(w=w):
                state_copy(w).start()

            @pl.when(w == seat)
            def _(w=w):
                held[w] = states[w]

    def local_step(head, carry):
        lanes = by_head(head)
        scores = None
        for way in (0, 1):
            part = jnp.where(masks[way], dot_nt(reach[way, :, lanes], scaled[way, :, lanes]), 0.0)
            scores = part if scores is None else scores + part
        locals_[:, lanes] = dot_nn(scores.astype(jnp.bfloat16), v_v[:, lanes])
        return carry

    lax.fori_loop(0, heads, local_step, 0)

    spread(1)
    onward(0)

    for w in range(side):
        @pl.when(w != seat)
        def _(w=w):
            state_arrival(w).wait_recv()

    back = seat // half

    def turn(i, count):
        return i + back * (count - 1 - 2 * i)

    def unpack(block):
        return block[:, width : width + 1] + block[:, width + 1 : width + 2], block[:, :width]

    entry[...] = jnp.zeros_like(entry)

    def first_pass(i, decay):
        factor, state = unpack(held[turn(i, side)].astype(jnp.float32))
        entry[...] = factor * entry[...] + state
        return factor * decay

    decay = lax.fori_loop(0, side, first_pass, jnp.ones((per, 1, width), jnp.float32))
    total[:, 0:width] = entry[...].astype(jnp.bfloat16)
    for i in range(per):
        total[i, width : width + PAD_ROWS] = pad(decay[i])

    def give_after(k):
        return (zs[k] > z) == (back == 0)

    def total_copy(k):
        return copy(total, totals_in.at[z], s2_out.at[k], s2_in.at[k], along[k])

    for k in range(1, nz):
        @pl.when(give_after(k))
        def _(k=k):
            total_copy(k).start()
    for one in first(late):
        one.start()
    entry[...] = jnp.zeros_like(entry)
    for k in range(1, nz):
        @pl.when(jnp.logical_not(give_after(k)))
        def _(k=k):
            total_copy(k).wait_recv()
    for i in range(nz):
        source = turn(i, nz)

        @pl.when(jnp.logical_and(source != z, (source < z) == (back == 0)))
        def _(source=source):
            factor, state = unpack(totals_in[source].astype(jnp.float32))
            entry[...] = factor * entry[...] + state

    def enter_copy(w):
        return copy(made.at[w], enter.at[seat], s3_out.at[w], s3_in.at[seat], base + w)

    def enter_arrival(w):
        return copy(made.at[w], enter.at[w], s3_out.at[w], s3_in.at[w], base + w)

    def second_pass(i, carry):
        source = turn(i, side)
        made[source] = entry[...].astype(jnp.bfloat16)

        @pl.when(source != seat)
        def _():
            enter_copy(source).start()

        factor, state = unpack(held[source].astype(jnp.float32))
        entry[...] = factor * entry[...] + state
        return carry

    lax.fori_loop(0, side, second_pass, 0)
    enter[seat] = made[seat]

    spread(2)
    onward(1)
    last(0)
    for load in loads[3:]:
        load.wait()
    for w in range(side):
        @pl.when(w != seat)
        def _(w=w):
            enter_arrival(w).wait_recv()

    def mix_step(head, carry):
        lanes = by_head(head)
        group, i = head // per, lax.rem(head, per)
        mix = (
            locals_[:, lanes]
            + dot_nt(reach[0, :, lanes], enter[group, i])
            + dot_nt(reach[1, :, lanes], enter[half + group, i])
        )
        scale = lax.rsqrt(jnp.mean(mix * mix, axis=-1, keepdims=True) + NORM_EPS)
        gate = silu(og_v[:, lanes].astype(jnp.float32))
        mixed[:, lanes] = (mix * scale * hgain_ref[...].astype(jnp.float32) * gate).astype(jnp.bfloat16)
        return carry

    lax.fori_loop(0, heads, mix_step, 0)
    chunk = 512 if columns % 512 == 0 else width

    def hidden_step(i, carry):
        lanes = pl.ds(pl.multiple_of(i * chunk, chunk), chunk)
        part = dot_nn(mixed[...], wo_v[:, lanes]).astype(jnp.bfloat16).astype(jnp.float32)
        hidden = (res_v[:, lanes].astype(jnp.float32) + part).astype(jnp.bfloat16)
        res_v[:, lanes] = hidden
        hidden = hidden.astype(jnp.float32)
        return carry + jnp.sum(hidden * hidden, axis=-1, keepdims=True)

    squares = lax.fori_loop(0, columns // chunk, hidden_step, jnp.zeros((rows, 1), jnp.float32))
    scale = lax.rsqrt(squares / columns + NORM_EPS)
    tok[z] = (res_v[...].astype(jnp.float32) * scale * mgain_ref[...].astype(jnp.float32)).astype(jnp.bfloat16)

    up_dev, dn_dev = me + side, me - side

    def up(zz):
        return copy(tok.at[zz], tok.at[zz], up_out.at[zz], up_in.at[zz], up_dev)

    def dn(zz):
        return copy(tok.at[zz], tok.at[zz], dn_out.at[zz], dn_in.at[zz], dn_dev)

    @pl.when(z < nz - 1)
    def _():
        up(z).start()

    @pl.when(z > 0)
    def _():
        dn(z).start()

    def relay(k):
        @pl.when(z - k >= 0)
        def _():
            up(z - k).wait_recv()

            @pl.when(z < nz - 1)
            def _():
                up(z - k).start()

        @pl.when(z + k < nz)
        def _():
            dn(z + k).wait_recv()

            @pl.when(z > 0)
            def _():
                dn(z + k).start()

    for k in range(3, nz):
        spread(k)
    for k in range(2, nz - 1):
        onward(k)
    relay(1)
    for k in range(1, nz - 1):
        last(k)
    onward(nz - 1)
    for k in range(2, nz):
        relay(k)
    last(nz - 1)
    for k in range(nz):
        for j in range(PLANE):
            partner(k, j).wait_recv()

    def give(k):
        return copy(parts.at[k], terms.at[k], r_out.at[k], r_in.at[k], along[k])

    def mixer(zz, slot):
        block = tok[zz]
        gate_act = dot_nn(block, w_v[0])
        up_act = dot_nn(block, w_v[1])
        inner = (silu(gate_act) * up_act).astype(jnp.bfloat16)
        parts[slot] = dot_nt(inner, w_v[2]).astype(jnp.bfloat16)

    def mixer_step(i, carry):
        k = lax.rem(i + 1, nz)
        zz = z
        for j in range(1, nz):
            zz = jnp.where(k == j, zs[j], zz)
        mixer(zz, k)

        for j in range(1, nz):
            @pl.when(k == j)
            def _(j=j):
                give(j).start()

        return carry

    lax.fori_loop(0, nz, mixer_step, 0)
    added = res_v[...].astype(jnp.float32) + parts[0].astype(jnp.float32)
    for k in range(1, nz):
        give(k).wait_recv()
        added = added + terms[k].astype(jnp.float32)
    out_ref[...] = added.astype(jnp.bfloat16)

    for k in range(1, nz):
        for one in first(k):
            one.wait_send()
        give(k).wait_send()

        @pl.when(give_after(k))
        def _(k=k):
            total_copy(k).wait_send()
    for k in range(nz):
        plane(k, (x_out, x_in), x_dev).wait_send()
        plane(k, (y_out, y_in), y_dev).wait_send()
        corner(k).wait_send()
        for j in range(PLANE):
            partner(k, j).wait_send()

        @pl.when(jnp.logical_and(z < nz - 1, k <= z))
        def _(k=k):
            up(k).wait_send()

        @pl.when(jnp.logical_and(z > 0, k >= z))
        def _(k=k):
            dn(k).wait_send()
    for w in range(side):
        @pl.when(w != seat)
        def _(w=w):
            state_copy(w).wait_send()
            enter_copy(w).wait_send()


def layer(queries, forget_logits, values, gate_logits, slack, spike, head_gain, output_weight, residual, mixer_gain, gate, up, down):
    n = lax.axis_size("sp")
    nz = n // (PLANE * CORES)
    rows, columns = queries.shape
    heads, width = spike.shape[1], head_gain.shape[0]
    depth, units = gate.shape[0], gate.shape[1] // nz
    side = PLANE * CORES
    per = 2 * heads // side
    bf16, f32 = jnp.bfloat16, jnp.float32
    anywhere = pl.BlockSpec(memory_space=pl.ANY)
    near = pl.BlockSpec(memory_space=pltpu.VMEM)
    dma = pltpu.SemaphoreType.DMA
    return pl.pallas_call(
        functools.partial(layer_kernel, nz),
        in_specs=[anywhere] * 5 + [near] * 4 + [anywhere] * 4,
        out_specs=near,
        out_shape=jax.ShapeDtypeStruct((rows, columns), bf16),
        scratch_shapes=[
            pltpu.VMEM((rows, columns), bf16),
            pltpu.VMEM((2, rows, columns), bf16),
            pltpu.VMEM((rows, columns), bf16),
            pltpu.VMEM((rows, columns), bf16),
            pltpu.VMEM((rows, columns), bf16),
            pltpu.VMEM(output_weight.shape, bf16),
            pltpu.VMEM((3, n * depth, units), bf16),
            pltpu.VMEM((2, rows, columns), bf16),
            pltpu.VMEM((2, rows, columns), bf16),
            pltpu.VMEM((rows, columns), f32),
            pltpu.VMEM((side, per, width + PAD_ROWS, width), bf16),
            pltpu.VMEM((side, per, width + PAD_ROWS, width), bf16),
            pltpu.VMEM((per, width + PAD_ROWS, width), bf16),
            pltpu.VMEM((nz, per, width + PAD_ROWS, width), bf16),
            pltpu.VMEM((per, width, width), f32),
            pltpu.VMEM((side, per, width, width), bf16),
            pltpu.VMEM((side, per, width, width), bf16),
            pltpu.VMEM((rows, columns), bf16),
            pltpu.VMEM((nz, rows, columns), bf16),
            pltpu.VMEM((nz, rows, columns), bf16),
            pltpu.VMEM((nz, rows, columns), bf16),
            dma((6,)),
            dma((3,)),
            dma((3, nz)),
            dma((3, nz)),
            dma((nz,)), dma((nz,)), dma((nz,)), dma((nz,)), dma((nz,)), dma((nz,)),
            dma((nz, PLANE)), dma((nz, PLANE)),
            dma((side,)), dma((side,)),
            dma((nz,)), dma((nz,)),
            dma((side,)), dma((side,)),
            dma((nz,)), dma((nz,)), dma((nz,)), dma((nz,)),
            dma((nz,)), dma((nz,)),
        ],
        compiler_params=pltpu.CompilerParams(
            collective_id=7, has_side_effects=True, vmem_limit_bytes=60 * 1024 * 1024
        ),
        name="layer",
    )(
        queries, forget_logits, values, gate_logits, residual, slack.reshape(1, columns), spike,
        head_gain.reshape(1, width), mixer_gain.reshape(1, columns), output_weight, gate, up, down.T,
    )


def local(
    queries,
    forget_logits,
    value_matrix,
    output_gate_logits,
    forget_slack,
    spike_log_forget,
    head_norm_gain,
    output_weight,
    residual,
    mixer_norm_gain,
    mixer_gate_weight,
    mixer_up_weight,
    mixer_down_weight,
):
    n, tp = lax.axis_size("sp"), lax.axis_size("tp")
    nz, tail = n // (PLANE * CORES), n % (PLANE * CORES)
    if tp == 1 and tail == 0 and nz in (2, 4) and mixer_gate_weight.shape[1] % (128 * nz) == 0:
        return layer(
            queries,
            forget_logits,
            value_matrix,
            output_gate_logits,
            forget_slack,
            spike_log_forget,
            head_norm_gain,
            output_weight,
            residual,
            mixer_norm_gain,
            mixer_gate_weight,
            mixer_up_weight,
            mixer_down_weight,
        )
    g = GROUP
    row_count = queries.shape[0]
    depth, units = mixer_gate_weight.shape
    far = [[b * g + j for b in range(n // g)] for j in range(g)]

    def cut(weight):
        return weight.reshape(depth, g, units // g).transpose(1, 0, 2)

    pieces = reshard([cut(mixer_gate_weight), cut(mixer_up_weight), cut(mixer_down_weight.T)], g, 2)
    gate_weight, up_weight, down_weight = (
        lax.all_gather(
            p.reshape(g * depth, units // g), "sp", axis=0, tiled=True, axis_index_groups=far
        )
        for p in pieces
    )

    local_out, reach, states = sweep(
        queries, forget_logits, value_matrix, forget_slack, spike_log_forget
    )
    entered = exchange(states)
    part = project(local_out, reach, entered, head_norm_gain, output_gate_logits, output_weight)
    part_rows = row_count // tp
    if tp > 1:
        part = lax.psum_scatter(part, "tp", scatter_dimension=0, tiled=True)
        residual = lax.dynamic_slice_in_dim(
            residual, lax.axis_index("tp") * part_rows, part_rows, 0
        )
    hidden = (residual.astype(jnp.float32) + part.astype(jnp.float32)).astype(jnp.bfloat16)
    hidden_f = hidden.astype(jnp.float32)
    normed = (
        hidden_f
        * lax.rsqrt(jnp.mean(hidden_f * hidden_f, axis=-1, keepdims=True) + NORM_EPS)
        * mixer_norm_gain.astype(jnp.float32)
    ).astype(jnp.bfloat16)
    normed = gather(normed, g, 4)
    if tp > 1:
        normed = lax.all_gather(normed, "tp", axis=0, tiled=True)
    gate_act = dot_nn(normed, gate_weight)
    up_act = dot_nn(normed, up_weight)
    inner = (silu(gate_act) * up_act).astype(jnp.bfloat16)
    lowered = dot_nt(inner, down_weight).astype(jnp.bfloat16)
    if tp > 1:
        lowered = lax.psum_scatter(lowered, "tp", scatter_dimension=0, tiled=True)
    (terms,) = reshard([lowered.reshape(g, part_rows, lowered.shape[1])], g, 3)
    added = jnp.sum(terms.astype(jnp.float32), axis=0)
    return (hidden_f + added).astype(jnp.bfloat16)


def solution(mesh):
    placed = (
        P("sp", "tp"),
        P(None, "sp", "tp"),
        P("sp", "tp"),
        P("sp", "tp"),
        P("tp"),
        P("sp", "tp"),
        P(),
        P("tp", None),
        P("sp", None),
        P(),
        P("sp", "tp"),
        P("sp", "tp"),
        P("tp", "sp"),
    )
    return jax.shard_map(
        local, mesh=mesh, in_specs=placed, out_specs=P(("sp", "tp"), None), check_vma=False
    )
```

```python
import functools

import jax
import jax.numpy as jnp
from jax import lax
from jax.experimental import pallas as pl
from jax.experimental.pallas import tpu as pltpu
from jax.sharding import PartitionSpec as P

NORM_EPS = 1e-06
MESH = pl.DeviceIdType.MESH
PAD_ROWS = 16
GROUP = 8


def dot_nt(a, b):
    return lax.dot_general(a, b, (((1,), (1,)), ((), ())), preferred_element_type=jnp.float32)


def dot_tn(a, b):
    return lax.dot_general(a, b, (((0,), (0,)), ((), ())), preferred_element_type=jnp.float32)


def dot_nn(a, b):
    return jnp.dot(a, b, preferred_element_type=jnp.float32)


def silu(x):
    return x * jax.nn.sigmoid(x)


def split_bf16(x):
    high = x.astype(jnp.bfloat16)
    return high, (x - high.astype(jnp.float32)).astype(jnp.bfloat16)


def sweep_kernel(q_ref, f_ref, v_ref, slack_ref, spike_ref, local_ref, reach_ref, state_ref):
    head = pl.program_id(0)
    rows, width = q_ref.shape
    query = silu(q_ref[...].astype(jnp.float32)) * (width ** -0.5)
    value = v_ref[...]
    spikes = spike_ref[...]
    lane = lax.broadcasted_iota(jnp.int32, spikes.shape, 1)
    spike = jnp.sum(jnp.where(lane == head, spikes, 0.0), axis=1, keepdims=True)
    slack = slack_ref[...]
    down = lax.broadcasted_iota(jnp.int32, (rows, rows), 0)
    across = lax.broadcasted_iota(jnp.int32, (rows, rows), 1)
    scores = None
    for way in (0, 1):
        mask = (down >= across) if way == 0 else (down <= across)
        tri = jnp.where(mask, 1.0, 0.0).astype(jnp.bfloat16)
        key = slack * jax.nn.sigmoid(-f_ref[way].astype(jnp.float32))
        decay = jnp.log1p(-key) + spike
        high, low = split_bf16(decay)
        running = dot_nn(tri, high) + dot_nn(tri, low)
        final = running[rows - 1 : rows] if way == 0 else running[0:1]
        query_scaled = (query * jnp.exp(running)).astype(jnp.bfloat16)
        key_scaled = (key * jnp.exp(-running)).astype(jnp.bfloat16)
        key_end = (key * jnp.exp(final - running)).astype(jnp.bfloat16)
        part = jnp.where(mask, dot_nt(query_scaled, key_scaled), 0.0)
        scores = part if scores is None else scores + part
        reach_ref[way] = query_scaled
        state_ref[way, 0, 0:width] = dot_tn(value, key_end).astype(jnp.bfloat16)
        total_high, total_low = split_bf16(jnp.exp(final))
        place = lax.broadcasted_iota(jnp.int32, (PAD_ROWS, width), 0)
        state_ref[way, 0, width : width + PAD_ROWS] = jnp.where(
            place == 0,
            total_high.astype(jnp.float32),
            jnp.where(place == 1, total_low.astype(jnp.float32), 0.0),
        ).astype(jnp.bfloat16)
    local_ref[...] = dot_nn(scores.astype(jnp.bfloat16), value)


def sweep(queries, forget_logits, values, slack, spike):
    rows, columns = queries.shape
    heads = spike.shape[1]
    width = columns // heads
    by_head = pl.BlockSpec((rows, width), lambda h: (0, h))
    return pl.pallas_call(
        sweep_kernel,
        grid=(heads,),
        in_specs=[
            by_head,
            pl.BlockSpec((2, rows, width), lambda h: (0, 0, h)),
            by_head,
            pl.BlockSpec((1, width), lambda h: (0, h)),
            pl.BlockSpec((rows, heads), lambda h: (0, 0)),
        ],
        out_specs=[
            by_head,
            pl.BlockSpec((2, rows, width), lambda h: (0, 0, h)),
            pl.BlockSpec((2, 1, width + PAD_ROWS, width), lambda h: (0, h, 0, 0)),
        ],
        out_shape=[
            jax.ShapeDtypeStruct((rows, columns), jnp.float32),
            jax.ShapeDtypeStruct((2, rows, columns), jnp.bfloat16),
            jax.ShapeDtypeStruct((2, heads, width + PAD_ROWS, width), jnp.bfloat16),
        ],
        cost_estimate=pl.CostEstimate(
            flops=20 * rows * width * columns, bytes_accessed=8 * rows * columns, transcendentals=8 * rows * columns
        ),
        name="sweep",
    )(queries, forget_logits, values, slack.reshape(1, columns), spike)


def greet(axis, others, count):
    barrier = pltpu.get_barrier_semaphore()

    def signal(k, carry):
        pl.semaphore_signal(barrier, inc=1, device_id={axis: others(k)}, device_id_type=MESH)
        return carry

    lax.fori_loop(1, count, signal, 0)
    pl.semaphore_wait(barrier, count - 1)


def exchange_kernel(n, state_ref, enter_ref, held, made, out_sem, in_sem, out_sem2, in_sem2):
    me = lax.axis_index("sp")
    rows = enter_ref.shape[1]

    def other(k):
        return lax.rem(me + k, n)

    greet("sp", other, n)

    def first(k):
        there = other(k)
        return pltpu.make_async_remote_copy(
            src_ref=state_ref.at[there],
            dst_ref=held.at[me],
            send_sem=out_sem.at[k],
            recv_sem=in_sem.at[k],
            device_id={"sp": there},
            device_id_type=MESH,
        )

    def second(k):
        there = other(k)
        return pltpu.make_async_remote_copy(
            src_ref=made.at[there],
            dst_ref=enter_ref.at[me],
            send_sem=out_sem2.at[k],
            recv_sem=in_sem2.at[k],
            device_id={"sp": there},
            device_id_type=MESH,
        )

    def go(copy):
        def start(k, carry):
            copy(k).start()
            return carry

        lax.fori_loop(1, n, start, 0)

    def end(copy):
        def wait(k, carry):
            copy(k).wait()
            return carry

        lax.fori_loop(1, n, wait, 0)

    go(first)
    held[me] = state_ref[me]
    end(first)
    backward = me // (n // 2)

    def step(i, total):
        source = i + backward * (n - 1 - 2 * i)
        made[source] = total.astype(jnp.bfloat16)
        block = held[source].astype(jnp.float32)
        factor = block[rows : rows + 1] + block[rows + 1 : rows + 2]
        return factor * total + block[:rows]

    lax.fori_loop(0, n, step, jnp.zeros(enter_ref.shape[1:], jnp.float32))
    go(second)
    enter_ref[me] = made[me]
    end(second)


def exchange(states):
    n = lax.axis_size("sp")
    ways, heads, padded, width = states.shape
    depth = padded - PAD_ROWS
    cuts = n // (ways * heads)
    rows = depth // cuts
    if cuts > 1:
        body = states[:, :, :depth].reshape(ways, heads, cuts, rows, width)
        tail = jnp.broadcast_to(
            states[:, :, None, depth:], (ways, heads, cuts, PAD_ROWS, width)
        )
        states = jnp.concatenate([body, tail], axis=3)
    entered = pl.pallas_call(
        functools.partial(exchange_kernel, n),
        in_specs=[pl.BlockSpec(memory_space=pltpu.VMEM)],
        out_specs=pl.BlockSpec(memory_space=pltpu.VMEM),
        out_shape=jax.ShapeDtypeStruct((n, rows, width), jnp.bfloat16),
        scratch_shapes=[
            pltpu.VMEM((n, rows + PAD_ROWS, width), jnp.bfloat16),
            pltpu.VMEM((n, rows, width), jnp.bfloat16),
            pltpu.SemaphoreType.DMA((n,)),
            pltpu.SemaphoreType.DMA((n,)),
            pltpu.SemaphoreType.DMA((n,)),
            pltpu.SemaphoreType.DMA((n,)),
        ],
        compiler_params=pltpu.CompilerParams(collective_id=1, has_side_effects=True),
        name="exchange",
    )(states.reshape(n, rows + PAD_ROWS, width))
    return entered.reshape(ways, heads, depth, width)


def reshard_kernel(g, *refs):
    count = (len(refs) - 3) // 2
    gives, takes = refs[:count], refs[count : 2 * count]
    out_sem, in_sem, own_sem = refs[2 * count :]
    me = lax.axis_index("sp")
    base = me // g * g
    seat = me - base

    def other(k):
        return lax.rem(seat + k, g)

    greet("sp", lambda k: base + other(k), g)
    copies = []
    for k in range(1, g):
        there = other(k)
        for i in range(count):
            copies.append(
                pltpu.make_async_remote_copy(
                    src_ref=gives[i].at[there],
                    dst_ref=takes[i].at[seat],
                    send_sem=out_sem.at[i, k],
                    recv_sem=in_sem.at[i, k],
                    device_id={"sp": base + there},
                    device_id_type=MESH,
                )
            )
            copies[-1].start()
    for i in range(count):
        copies.append(pltpu.make_async_copy(gives[i].at[seat], takes[i].at[seat], own_sem.at[i]))
        copies[-1].start()
    for copy in copies:
        copy.wait()


def reshard(arrays, g, collective_id):
    count = len(arrays)
    return pl.pallas_call(
        functools.partial(reshard_kernel, g),
        in_specs=[pl.BlockSpec(memory_space=pltpu.VMEM)] * count,
        out_specs=[pl.BlockSpec(memory_space=pltpu.VMEM)] * count,
        out_shape=[jax.ShapeDtypeStruct(a.shape, a.dtype) for a in arrays],
        scratch_shapes=[
            pltpu.SemaphoreType.DMA((count, g)),
            pltpu.SemaphoreType.DMA((count, g)),
            pltpu.SemaphoreType.DMA((count,)),
        ],
        compiler_params=pltpu.CompilerParams(
            collective_id=collective_id, has_side_effects=True
        ),
        name="reshard",
    )(*arrays)


def gather_kernel(g, give, take, out_sem, in_sem):
    me = lax.axis_index("sp")
    base = me // g * g
    seat = me - base

    def other(k):
        return lax.rem(seat + k, g)

    greet("sp", lambda k: base + other(k), g)
    copies = []
    for k in range(1, g):
        copies.append(
            pltpu.make_async_remote_copy(
                src_ref=give,
                dst_ref=take.at[seat],
                send_sem=out_sem.at[k],
                recv_sem=in_sem.at[k],
                device_id={"sp": base + other(k)},
                device_id_type=MESH,
            )
        )
        copies[-1].start()
    take[seat] = give[...]
    for copy in copies:
        copy.wait()


def gather(array, g, collective_id):
    return pl.pallas_call(
        functools.partial(gather_kernel, g),
        in_specs=[pl.BlockSpec(memory_space=pltpu.VMEM)],
        out_specs=pl.BlockSpec(memory_space=pltpu.VMEM),
        out_shape=jax.ShapeDtypeStruct((g,) + array.shape, array.dtype),
        scratch_shapes=[pltpu.SemaphoreType.DMA((g,)), pltpu.SemaphoreType.DMA((g,))],
        compiler_params=pltpu.CompilerParams(
            collective_id=collective_id, has_side_effects=True
        ),
        name="gather",
    )(array).reshape((g * array.shape[0],) + array.shape[1:])


def project_kernel(local_ref, reach_ref, enter_ref, gain_ref, gate_ref, weight_ref, out_ref, total):
    head = pl.program_id(0)
    mix = (
        local_ref[...]
        + dot_nt(reach_ref[0], enter_ref[0, 0])
        + dot_nt(reach_ref[1], enter_ref[1, 0])
    )
    scale = lax.rsqrt(jnp.mean(mix * mix, axis=-1, keepdims=True) + NORM_EPS)
    gate = silu(gate_ref[...].astype(jnp.float32))
    mixed = (mix * scale * gain_ref[...].astype(jnp.float32) * gate).astype(jnp.bfloat16)
    term = dot_nn(mixed, weight_ref[...])

    @pl.when(head == 0)
    def _():
        total[...] = term

    @pl.when(head > 0)
    def _():
        total[...] += term

    @pl.when(head == pl.num_programs(0) - 1)
    def _():
        out_ref[...] = total[...].astype(jnp.bfloat16)


def project(local, reach, entered, gain, gate_logits, weight):
    rows, columns = local.shape
    heads, width = entered.shape[1], entered.shape[3]
    model = weight.shape[1]
    by_head = pl.BlockSpec((rows, width), lambda h: (0, h))
    return pl.pallas_call(
        project_kernel,
        grid=(heads,),
        in_specs=[
            by_head,
            pl.BlockSpec((2, rows, width), lambda h: (0, 0, h)),
            pl.BlockSpec((2, 1, width, width), lambda h: (0, h, 0, 0)),
            pl.BlockSpec((1, width), lambda h: (0, 0)),
            by_head,
            pl.BlockSpec((width, model), lambda h: (h, 0)),
        ],
        out_specs=pl.BlockSpec((rows, model), lambda h: (0, 0)),
        out_shape=jax.ShapeDtypeStruct((rows, model), jnp.bfloat16),
        scratch_shapes=[pltpu.VMEM((rows, model), jnp.float32)],
        cost_estimate=pl.CostEstimate(
            flops=2 * rows * columns * model, bytes_accessed=2 * columns * model, transcendentals=rows * columns
        ),
        name="project",
    )(local, reach, entered, gain.reshape(1, width), gate_logits, weight)


CORES = 2
PLANE = 4


def flip(i, k):
    out, bit = i, 1
    while bit <= k:
        if k & bit:
            out = out + bit - 2 * bit * (lax.rem(i // bit, 2))
        bit *= 2
    return out


def layer_kernel(
    nz,
    q_hbm, f_hbm, v_hbm, og_hbm, res_hbm, slack_ref, spike_ref, hgain_ref, mgain_ref, wo_hbm, gate_hbm, up_hbm, down_hbm,
    out_ref,
    q_v, f_v, v_v, og_v, res_v, wo_v, w_v,
    reach, scaled, locals_, states, mate, chip, held, total, totals_in, entry, made, enter, beside, mixed, tok, inner,
    parts, terms,
    in_sem, w0_sem, w1_out, w1_in, x_out, x_in, y_out, y_in, d_out, d_in, p_out, p_in,
    s0_out, s0_in, s1_out, s1_in, s2_out, s2_in, s3_out, s3_in, s4_out, s4_in,
    up_out, up_in, dn_out, dn_in, r_out, r_in,
):
    rows, columns = q_v.shape
    width = hgain_ref.shape[1]
    heads = columns // width
    depth = gate_hbm.shape[0]
    units = w_v.shape[2]
    side = PLANE * CORES
    per = heads // PLANE
    me = lax.axis_index("sp")
    z, seat = me // side, lax.rem(me, side)
    q, c = seat // CORES, lax.rem(seat, CORES)

    def at(zz, qq, cc):
        return zz * side + qq * CORES + cc

    def copy(src, dst, out_sem, got_sem, there):
        return pltpu.make_async_remote_copy(
            src_ref=src, dst_ref=dst, send_sem=out_sem, recv_sem=got_sem,
            device_id={"sp": there}, device_id_type=MESH,
        )

    def when(condition, act):
        pl.when(condition)(act)

    zs = [z] + [flip(z, k) for k in range(1, nz)]
    qs = [q] + [flip(q, k) for k in range(1, PLANE)]
    along = [at(zz, q, c) for zz in zs]
    x_dev, y_dev, p_dev = at(z, qs[1], c), at(z, qs[2], c), at(z, q, 1 - c)
    up_dev, dn_dev = me + side, me - side

    loads = [
        pltpu.make_async_copy(src, dst, in_sem.at[i])
        for i, (src, dst) in enumerate(
            ((f_hbm, f_v), (q_hbm, q_v), (v_hbm, v_v), (og_hbm, og_v), (res_hbm, res_v), (wo_hbm, wo_v))
        )
    ]
    weights = (gate_hbm, up_hbm, down_hbm)

    def cut(a, zz):
        return weights[a].at[:, pl.ds(pl.multiple_of(zz * units, 128), units)]

    def strip(a, device):
        return w_v.at[a, pl.ds(pl.multiple_of(device * depth, depth), depth), :]

    own = [pltpu.make_async_copy(cut(a, z), strip(a, me), w0_sem.at[a]) for a in range(3)]
    for load in loads[:3]:
        load.start()
    for load in own:
        load.start()

    barrier = pltpu.get_barrier_semaphore()
    for k in range(1, nz):
        pl.semaphore_signal(barrier, inc=1, device_id={"sp": along[k]}, device_id_type=MESH)
    for k in range(1, side):
        pl.semaphore_signal(
            barrier, inc=1, device_id={"sp": z * side + lax.rem(seat + k, side)}, device_id_type=MESH
        )
    pl.semaphore_wait(barrier, nz - 1 + side - 1)

    members = ((0, 1), (2,))

    outer = jnp.logical_or(z == 0, z == nz - 1)
    order = [z] + [jnp.where(outer, zs[i], zs[j]) for i, j in ((1, 2), (3, 1), (2, 3))]

    def source(part, k):
        return order[k] if part == 0 else k

    def first(part, k):
        return [
            copy(cut(a, zs[k]), strip(a, me), w1_out.at[0], w1_in.at[a, z], along[k]) for a in members[part]
        ]

    def first_start(*which):
        for part, k in which:
            for one in first(part, k):
                one.start()

    def first_wait(part, k):
        origin = source(part, k)

        @pl.when(origin != z)
        def _():
            for a in members[part]:
                copy(cut(a, z), strip(a, me), w1_out.at[0], w1_in.at[a, origin], along[1]).wait_recv()

    def piece(part, k, j):
        row = pl.multiple_of(at(source(part, k), qs[j], c) * depth, depth)
        lo, count = members[part][0], len(members[part])
        return w_v.at[pl.ds(lo, count), pl.ds(row, depth), :]

    def across_x(part, k):
        src = piece(part, k, 0)
        return copy(src, src, x_out.at[0], x_in.at[part, k], x_dev)

    def across_y(part, k):
        src = piece(part, k, 0)
        return copy(src, src, y_out.at[0], y_in.at[part, k], y_dev)

    def corner(part, k):
        near, there = (1, y_dev) if k < nz // 2 else (2, x_dev)
        src = piece(part, k, near)
        return copy(src, src, d_out.at[0], d_in.at[part, k], there)

    def partner(part, k, j):
        src = piece(part, k, j)
        return copy(src, src, p_out.at[0], p_in.at[part, k, j], p_dev)

    def spread(part, k):
        if part == 0 and k == 0:
            for a in members[0]:
                own[a].wait()
        else:
            first_wait(part, k)
        across_x(part, k).start()
        across_y(part, k).start()
        partner(part, k, 0).start()

    def onward(part, k):
        across_x(part, k).wait_recv()
        if k < nz // 2:
            corner(part, k).start()
        partner(part, k, 1).start()
        across_y(part, k).wait_recv()
        if k >= nz // 2:
            corner(part, k).start()
        partner(part, k, 2).start()

    def last(part, k):
        corner(part, k).wait_recv()
        partner(part, k, 3).start()

    def settle(part, k):
        for j in range(PLANE):
            partner(part, k, j).wait_recv()

    when(outer, lambda: first_start((0, 2), (0, 3)))
    when(jnp.logical_not(outer), lambda: first_start((0, 1)))
    spread(0, 0)
    for load in loads[3:]:
        load.start()

    down = lax.broadcasted_iota(jnp.int32, (rows, rows), 0)
    sideways = lax.broadcasted_iota(jnp.int32, (rows, rows), 1)
    masks = (down >= sideways, down <= sideways)
    for load in loads[:3]:
        load.wait()
    spikes = jnp.transpose(spike_ref[...])
    lane = lax.broadcasted_iota(jnp.int32, spikes.shape, 1)
    place = lax.broadcasted_iota(jnp.int32, (PAD_ROWS, width), 0)

    def pad(decay):
        high, low = split_bf16(decay)
        return jnp.where(
            place == 0, high.astype(jnp.float32), jnp.where(place == 1, low.astype(jnp.float32), 0.0)
        ).astype(jnp.bfloat16)

    def unpack(block):
        block = block.astype(jnp.float32)
        return block[:, width : width + 1] + block[:, width + 1 : width + 2], block[:, :width]

    def by_head(head):
        return pl.ds(pl.multiple_of(head * width, width), width)

    def make_states(group):
        def step(i, carry):
            head = group * per + i
            lanes = by_head(head)
            query = silu(q_v[:, lanes].astype(jnp.float32)) * (width ** -0.5)
            value = v_v[:, lanes]
            spike = jnp.sum(jnp.where(lane == head, spikes, 0.0), axis=1, keepdims=True)
            slack = slack_ref[:, lanes]
            for way in (0, 1):
                tri = jnp.where(masks[way], 1.0, 0.0).astype(jnp.bfloat16)
                key = slack * jax.nn.sigmoid(-f_v[way, :, lanes].astype(jnp.float32))
                decay = jnp.log1p(-key) + spike
                high, low = split_bf16(decay)
                running = dot_nn(tri, high) + dot_nn(tri, low)
                final = running[rows - 1 : rows] if way == 0 else running[0:1]
                reach[way, :, lanes] = (query * jnp.exp(running)).astype(jnp.bfloat16)
                scaled[way, :, lanes] = (key * jnp.exp(-running)).astype(jnp.bfloat16)
                key_end = (key * jnp.exp(final - running)).astype(jnp.bfloat16)
                states[way, group, i, 0:width] = dot_tn(value, key_end).astype(jnp.bfloat16)
                states[way, group, i, width : width + PAD_ROWS] = pad(jnp.exp(final))
            return carry

        lax.fori_loop(0, per, step, 0)

    def mate_copy(group):
        return copy(states.at[1 - c, group], mate.at[group], s0_out.at[group], s0_in.at[group], p_dev)

    def chip_copy(group):
        return copy(chip.at[group], held.at[q], s1_out.at[group], s1_in.at[q], at(z, group, c))

    def chip_arrival(group):
        return copy(chip.at[group], held.at[group], s1_out.at[group], s1_in.at[group], at(z, group, c))

    def join(group):
        mate_copy(group).wait_recv()
        factor, state = unpack(states[c, group])
        mate_factor, mate_state = unpack(mate[group])
        chip[group, :, 0:width] = (mate_factor * state + mate_state).astype(jnp.bfloat16)
        both = factor * mate_factor
        for i in range(per):
            chip[group, i, width : width + PAD_ROWS] = pad(both[i])
        when(q != group, lambda: chip_copy(group).start())

        @pl.when(q == group)
        def _():
            held[group] = chip[group]

    def local_step(head, carry):
        lanes = by_head(head)
        scores = None
        for way in (0, 1):
            part = jnp.where(masks[way], dot_nt(reach[way, :, lanes], scaled[way, :, lanes]), 0.0)
            scores = part if scores is None else scores + part
        locals_[:, lanes] = dot_nn(scores.astype(jnp.bfloat16), v_v[:, lanes])
        return carry

    for group in range(PLANE):
        make_states(group)
        mate_copy(group).start()
        if group > 0:
            join(group - 1)
    lax.fori_loop(0, heads // 2, local_step, 0)
    join(PLANE - 1)
    lax.fori_loop(heads // 2, heads, local_step, 0)
    onward(0, 0)

    for w in range(PLANE):
        when(w != q, lambda w=w: chip_arrival(w).wait_recv())

    def turn(i, count):
        return i + c * (count - 1 - 2 * i)

    entry[...] = jnp.zeros_like(entry)
    decay = jnp.ones((per, 1, width), jnp.float32)
    for i in range(PLANE):
        factor, state = unpack(held[turn(i, PLANE)])
        entry[...] = factor * entry[...] + state
        decay = factor * decay
    total[:, 0:width] = entry[...].astype(jnp.bfloat16)
    for i in range(per):
        total[i, width : width + PAD_ROWS] = pad(decay[i])

    def give_after(k):
        return (zs[k] > z) == (c == 0)

    def total_copy(k):
        return copy(total, totals_in.at[z], s2_out.at[k], s2_in.at[k], along[k])

    for k in range(1, nz):
        when(give_after(k), lambda k=k: total_copy(k).start())
    when(outer, lambda: first_start((0, 1)))
    own[2].wait()
    when(jnp.logical_not(outer), lambda: first_start((0, 3), (0, 2), (1, 1), (1, 3), (1, 2)))
    spread(0, 1)
    entry[...] = jnp.zeros_like(entry)
    for k in range(1, nz):
        when(jnp.logical_not(give_after(k)), lambda k=k: total_copy(k).wait_recv())
    for i in range(nz):
        origin = turn(i, nz)

        @pl.when(jnp.logical_and(origin != z, (origin < z) == (c == 0)))
        def _(origin=origin):
            factor, state = unpack(totals_in[origin])
            entry[...] = factor * entry[...] + state

    def enter_copy(w):
        return copy(made.at[w], enter.at[c, q], s3_out.at[w], s3_in.at[q], at(z, w, c))

    def enter_arrival(w):
        return copy(made.at[w], enter.at[c, w], s3_out.at[w], s3_in.at[w], at(z, w, c))

    def beside_copy(group):
        return copy(beside.at[group], enter.at[c, group], s4_out.at[group], s4_in.at[group], p_dev)

    def beside_arrival(group):
        return copy(beside.at[group], enter.at[1 - c, group], s4_out.at[group], s4_in.at[group], p_dev)

    for i in range(PLANE):
        origin = turn(i, PLANE)
        made[origin] = entry[...].astype(jnp.bfloat16)
        when(origin != q, lambda origin=origin: enter_copy(origin).start())
        factor, state = unpack(held[origin])
        entry[...] = factor * entry[...] + state
    enter[c, q] = made[q]
    onward(0, 1)
    when(outer, lambda: first_start((1, 2), (1, 3), (1, 1)))
    last(0, 0)
    spread(0, 2)
    for w in range(PLANE):
        when(w != q, lambda w=w: enter_arrival(w).wait_recv())
        factor, state = unpack(states[c, w])
        beside[w] = (factor * enter[c, w].astype(jnp.float32) + state).astype(jnp.bfloat16)
        beside_copy(w).start()
    for load in loads[3:]:
        load.wait()
    for w in range(PLANE):
        beside_arrival(w).wait_recv()

    def mix_step(head, carry):
        lanes = by_head(head)
        group, i = head // per, lax.rem(head, per)
        mix = (
            locals_[:, lanes]
            + dot_nt(reach[0, :, lanes], enter[0, group, i])
            + dot_nt(reach[1, :, lanes], enter[1, group, i])
        )
        scale = lax.rsqrt(jnp.mean(mix * mix, axis=-1, keepdims=True) + NORM_EPS)
        gate = silu(og_v[:, lanes].astype(jnp.float32))
        mixed[:, lanes] = (mix * scale * hgain_ref[...].astype(jnp.float32) * gate).astype(jnp.bfloat16)
        return carry

    lax.fori_loop(0, heads, mix_step, 0)
    chunk = columns // nz

    def hidden_step(i, carry):
        lanes = pl.ds(pl.multiple_of(i * chunk, chunk), chunk)
        part = dot_nn(mixed[...], wo_v[:, lanes]).astype(jnp.bfloat16).astype(jnp.float32)
        hidden = (res_v[:, lanes].astype(jnp.float32) + part).astype(jnp.bfloat16)
        res_v[:, lanes] = hidden
        hidden = hidden.astype(jnp.float32)
        return carry + jnp.sum(hidden * hidden, axis=-1, keepdims=True)

    squares = lax.fori_loop(0, columns // chunk, hidden_step, jnp.zeros((rows, 1), jnp.float32))
    scale = lax.rsqrt(squares / columns + NORM_EPS)
    for i in range(columns // width):
        lanes = pl.ds(i * width, width)
        gain = mgain_ref[i : i + 1].astype(jnp.float32)
        tok[z, :, lanes] = (res_v[:, lanes].astype(jnp.float32) * scale * gain).astype(jnp.bfloat16)

    def half(zz, h):
        return tok.at[zz, :, pl.ds(h * (columns // 2), columns // 2)]

    def up(zz, h):
        return copy(half(zz, h), half(zz, h), up_out.at[zz, h], up_in.at[zz, h], up_dev)

    def dn(zz, h):
        return copy(half(zz, h), half(zz, h), dn_out.at[zz, h], dn_in.at[zz, h], dn_dev)

    for h in (0, 1):
        when(z < nz - 1, lambda h=h: up(z, h).start())
        when(z > 0, lambda h=h: dn(z, h).start())

    def relay(k, h):
        @pl.when(z - k >= 0)
        def _():
            up(z - k, h).wait_recv()
            when(z < nz - 1, lambda: up(z - k, h).start())

        @pl.when(z + k < nz)
        def _():
            dn(z + k, h).wait_recv()
            when(z > 0, lambda: dn(z + k, h).start())

    def expand(zz):
        block = tok[zz]
        gate_act = dot_nn(block, w_v[0])
        up_act = dot_nn(block, w_v[1])
        inner[zz] = (silu(gate_act) * up_act).astype(jnp.bfloat16)

    def ordered(i):
        reach_dn, reach_up = z, nz - 1 - z
        near = jnp.minimum(reach_dn, reach_up)
        pair = (i + 1) // 2
        odd = lax.rem(i, 2)
        both = z + jnp.where(odd == 1, -pair, pair)
        single = jnp.where(reach_dn < reach_up, i, nz - 1 - i)
        return jnp.where(pair <= near, both, single)

    def lanes_of(s):
        return pl.ds(s * chunk, chunk)

    def lower(zz, s):
        out = dot_nt(inner[zz], w_v[2, s * chunk : (s + 1) * chunk])
        parts[zz, :, lanes_of(s)] = out.astype(jnp.bfloat16)

    def sum_up(zz, s):
        return copy(
            parts.at[zz, :, lanes_of(s)], terms.at[0, zz, :, lanes_of(s)], r_out.at[0], r_in.at[0, zz, s], up_dev
        )

    def sum_dn(zz, s):
        return copy(
            parts.at[zz, :, lanes_of(s)], terms.at[1, zz, :, lanes_of(s)], r_out.at[0], r_in.at[1, zz, s], dn_dev
        )

    def take(way, zz, s):
        (sum_up, sum_dn)[way](zz, s).wait_recv()
        parts[zz, :, lanes_of(s)] = (
            parts[zz, :, lanes_of(s)].astype(jnp.float32) + terms[way, zz, :, lanes_of(s)].astype(jnp.float32)
        ).astype(jnp.bfloat16)

    def ends(s, *far):
        for d in far:
            when(z == 0, lambda d=d: sum_up(d, s).start())
            when(z == nz - 1, lambda d=d: sum_dn(nz - 1 - d, s).start())

    def pass_up(at_z, zz, s):
        @pl.when(z == at_z)
        def _():
            take(0, zz, s)
            sum_up(zz, s).start()

    def pass_dn(at_z, zz, s):
        @pl.when(z == at_z)
        def _():
            take(1, zz, s)
            sum_dn(zz, s).start()

    def near_pass(s):
        pass_up(1, 2, s)
        pass_dn(2, 1, s)

    def far_pass(s):
        pass_up(1, 3, s)
        pass_dn(2, 0, s)

    def end_pass(s):
        pass_up(2, 3, s)
        pass_dn(1, 0, s)

    def work(lo, hi, act):
        def step(i, carry):
            act(ordered(i))
            return carry

        lax.fori_loop(lo, hi, step, 0)

    spread(0, 3)
    onward(0, 2)
    spread(1, 0)
    last(0, 1)
    relay(1, 0)
    onward(0, 3)
    spread(1, 1)
    last(0, 2)
    settle(0, 0)
    settle(0, 1)
    relay(1, 1)
    onward(1, 0)
    spread(1, 2)
    last(0, 3)
    relay(2, 0)
    settle(0, 2)
    settle(0, 3)
    work(0, 1, expand)
    onward(1, 1)
    spread(1, 3)
    work(1, 2, expand)
    relay(2, 1)
    last(1, 0)
    work(2, 3, expand)
    settle(1, 0)
    work(0, 3, lambda zz: lower(zz, 0))
    ends(0, 1, 2)
    onward(1, 2)
    last(1, 1)
    settle(1, 1)
    work(0, 3, lambda zz: lower(zz, 1))
    ends(1, 1, 2)
    near_pass(0)
    onward(1, 3)
    last(1, 2)
    settle(1, 2)
    work(0, 3, lambda zz: lower(zz, 2))
    ends(2, 1, 2)
    near_pass(1)
    relay(3, 0)
    relay(3, 1)
    work(3, 4, expand)
    for s in range(3):
        work(3, 4, lambda zz, s=s: lower(zz, s))
        ends(s, 3)
    last(1, 3)
    settle(1, 3)
    near_pass(2)
    far_pass(0)
    work(0, 4, lambda zz: lower(zz, 3))
    ends(3, 3, 2, 1)
    far_pass(1)
    end_pass(0)
    far_pass(2)
    end_pass(1)
    far_pass(3)
    near_pass(3)
    end_pass(2)
    end_pass(3)

    def finish(s):
        when(z > 0, lambda: sum_up(z, s).wait_recv())
        when(z < nz - 1, lambda: sum_dn(z, s).wait_recv())
        lanes = lanes_of(s)
        added = res_v[:, lanes].astype(jnp.float32) + parts[z, :, lanes].astype(jnp.float32)
        added = added + jnp.where(z > 0, terms[0, z, :, lanes].astype(jnp.float32), 0.0)
        added = added + jnp.where(z < nz - 1, terms[1, z, :, lanes].astype(jnp.float32), 0.0)
        out_ref[:, lanes] = added.astype(jnp.bfloat16)

    for s in range(nz):
        finish(s)

    def sent(src, sem, got_sem, there):
        copy(src, src, sem, got_sem, there).wait_send()

    sent(w_v.at[:, 0 : (nz - 1) * depth], w1_out.at[0], w1_in.at[0, 0], x_dev)
    sent(w_v.at[:, 0 : nz * depth], x_out.at[0], x_in.at[0, 0], x_dev)
    sent(w_v.at[:, 0 : nz * depth], y_out.at[0], y_in.at[0, 0], y_dev)
    sent(w_v.at[:, 0 : nz * depth], d_out.at[0], d_in.at[0, 0], x_dev)
    sent(w_v.at[:, 0 : PLANE * nz * depth], p_out.at[0], p_in.at[0, 0, 0], p_dev)
    sent(parts.at[0 : nz - 1], r_out.at[0], r_in.at[0, 0, 0], x_dev)
    for k in range(1, nz):
        when(give_after(k), lambda k=k: total_copy(k).wait_send())
    for k in range(nz):
        for h in (0, 1):
            when(jnp.logical_and(z < nz - 1, k <= z), lambda k=k, h=h: up(k, h).wait_send())
            when(jnp.logical_and(z > 0, k >= z), lambda k=k, h=h: dn(k, h).wait_send())
    for w in range(PLANE):
        mate_copy(w).wait_send()
        beside_copy(w).wait_send()

        @pl.when(w != q)
        def _(w=w):
            chip_copy(w).wait_send()
            enter_copy(w).wait_send()


def layer(queries, forget_logits, values, gate_logits, slack, spike, head_gain, output_weight, residual, mixer_gain, gate, up, down):
    n = lax.axis_size("sp")
    nz = n // (PLANE * CORES)
    rows, columns = queries.shape
    heads, width = spike.shape[1], head_gain.shape[0]
    depth, units = gate.shape[0], gate.shape[1] // nz
    per = heads // PLANE
    bf16, f32 = jnp.bfloat16, jnp.float32
    anywhere = pl.BlockSpec(memory_space=pl.ANY)
    near = pl.BlockSpec(memory_space=pltpu.VMEM)
    dma = pltpu.SemaphoreType.DMA
    padded = width + PAD_ROWS

    def pairs(*shape):
        return [dma(shape), dma(shape)]

    def one_out(*shape):
        return [dma((1,)), dma(shape)]

    return pl.pallas_call(
        functools.partial(layer_kernel, nz),
        in_specs=[anywhere] * 5 + [near] * 4 + [anywhere] * 4,
        out_specs=near,
        out_shape=jax.ShapeDtypeStruct((rows, columns), bf16),
        scratch_shapes=[
            pltpu.VMEM((rows, columns), bf16),
            pltpu.VMEM((2, rows, columns), bf16),
            pltpu.VMEM((rows, columns), bf16),
            pltpu.VMEM((rows, columns), bf16),
            pltpu.VMEM((rows, columns), bf16),
            pltpu.VMEM(output_weight.shape, bf16),
            pltpu.VMEM((3, n * depth, units), bf16),
            pltpu.VMEM((2, rows, columns), bf16),
            pltpu.VMEM((2, rows, columns), bf16),
            pltpu.VMEM((rows, columns), f32),
            pltpu.VMEM((2, PLANE, per, padded, width), bf16),
            pltpu.VMEM((PLANE, per, padded, width), bf16),
            pltpu.VMEM((PLANE, per, padded, width), bf16),
            pltpu.VMEM((PLANE, per, padded, width), bf16),
            pltpu.VMEM((per, padded, width), bf16),
            pltpu.VMEM((nz, per, padded, width), bf16),
            pltpu.VMEM((per, width, width), f32),
            pltpu.VMEM((PLANE, per, width, width), bf16),
            pltpu.VMEM((2, PLANE, per, width, width), bf16),
            pltpu.VMEM((PLANE, per, width, width), bf16),
            pltpu.VMEM((rows, columns), bf16),
            pltpu.VMEM((nz, rows, columns), bf16),
            pltpu.VMEM((nz, rows, units), bf16),
            pltpu.VMEM((nz, rows, columns), bf16),
            pltpu.VMEM((2, nz, rows, columns), bf16),
            dma((6,)),
            dma((3,)),
            *one_out(3, nz),
            *one_out(2, nz),
            *one_out(2, nz),
            *one_out(2, nz),
            *one_out(2, nz, PLANE),
            *pairs(PLANE),
            *pairs(PLANE),
            *pairs(nz),
            *pairs(PLANE),
            *pairs(PLANE),
            *pairs(nz, 2),
            *pairs(nz, 2),
            *one_out(2, nz, nz),
        ],
        compiler_params=pltpu.CompilerParams(
            collective_id=7, has_side_effects=True, vmem_limit_bytes=60 * 1024 * 1024
        ),
        name="layer",
    )(
        queries, forget_logits, values, gate_logits, residual, slack.reshape(1, columns), spike.T,
        head_gain.reshape(1, width), mixer_gain.reshape(columns // width, width), output_weight, gate, up, down.T,
    )


def local(
    queries,
    forget_logits,
    value_matrix,
    output_gate_logits,
    forget_slack,
    spike_log_forget,
    head_norm_gain,
    output_weight,
    residual,
    mixer_norm_gain,
    mixer_gate_weight,
    mixer_up_weight,
    mixer_down_weight,
):
    n, tp = lax.axis_size("sp"), lax.axis_size("tp")
    nz, tail = n // (PLANE * CORES), n % (PLANE * CORES)
    if tp == 1 and tail == 0 and nz == PLANE and mixer_gate_weight.shape[1] % (128 * nz) == 0:
        return layer(
            queries,
            forget_logits,
            value_matrix,
            output_gate_logits,
            forget_slack,
            spike_log_forget,
            head_norm_gain,
            output_weight,
            residual,
            mixer_norm_gain,
            mixer_gate_weight,
            mixer_up_weight,
            mixer_down_weight,
        )
    g = GROUP
    row_count = queries.shape[0]
    depth, units = mixer_gate_weight.shape
    far = [[b * g + j for b in range(n // g)] for j in range(g)]

    def cut(weight):
        return weight.reshape(depth, g, units // g).transpose(1, 0, 2)

    pieces = reshard([cut(mixer_gate_weight), cut(mixer_up_weight), cut(mixer_down_weight.T)], g, 2)
    gate_weight, up_weight, down_weight = (
        lax.all_gather(
            p.reshape(g * depth, units // g), "sp", axis=0, tiled=True, axis_index_groups=far
        )
        for p in pieces
    )

    local_out, reach, states = sweep(
        queries, forget_logits, value_matrix, forget_slack, spike_log_forget
    )
    entered = exchange(states)
    part = project(local_out, reach, entered, head_norm_gain, output_gate_logits, output_weight)
    part_rows = row_count // tp
    if tp > 1:
        part = lax.psum_scatter(part, "tp", scatter_dimension=0, tiled=True)
        residual = lax.dynamic_slice_in_dim(
            residual, lax.axis_index("tp") * part_rows, part_rows, 0
        )
    hidden = (residual.astype(jnp.float32) + part.astype(jnp.float32)).astype(jnp.bfloat16)
    hidden_f = hidden.astype(jnp.float32)
    normed = (
        hidden_f
        * lax.rsqrt(jnp.mean(hidden_f * hidden_f, axis=-1, keepdims=True) + NORM_EPS)
        * mixer_norm_gain.astype(jnp.float32)
    ).astype(jnp.bfloat16)
    normed = gather(normed, g, 4)
    if tp > 1:
        normed = lax.all_gather(normed, "tp", axis=0, tiled=True)
    gate_act = dot_nn(normed, gate_weight)
    up_act = dot_nn(normed, up_weight)
    inner = (silu(gate_act) * up_act).astype(jnp.bfloat16)
    lowered = dot_nt(inner, down_weight).astype(jnp.bfloat16)
    if tp > 1:
        lowered = lax.psum_scatter(lowered, "tp", scatter_dimension=0, tiled=True)
    (terms,) = reshard([lowered.reshape(g, part_rows, lowered.shape[1])], g, 3)
    added = jnp.sum(terms.astype(jnp.float32), axis=0)
    return (hidden_f + added).astype(jnp.bfloat16)


def solution(mesh):
    placed = (
        P("sp", "tp"),
        P(None, "sp", "tp"),
        P("sp", "tp"),
        P("sp", "tp"),
        P("tp"),
        P("sp", "tp"),
        P(),
        P("tp", None),
        P("sp", None),
        P(),
        P("sp", "tp"),
        P("sp", "tp"),
        P("tp", "sp"),
    )
    return jax.shard_map(
        local, mesh=mesh, in_specs=placed, out_specs=P(("sp", "tp"), None), check_vma=False
    )
```

```python
import functools

import jax
import jax.numpy as jnp
from jax import lax
from jax.experimental import pallas as pl
from jax.experimental.pallas import tpu as pltpu
from jax.sharding import PartitionSpec as P

NORM_EPS = 1e-06
MESH = pl.DeviceIdType.MESH
PAD_ROWS = 16
GROUP = 8


def dot_nt(a, b):
    return lax.dot_general(a, b, (((1,), (1,)), ((), ())), preferred_element_type=jnp.float32)


def dot_tn(a, b):
    return lax.dot_general(a, b, (((0,), (0,)), ((), ())), preferred_element_type=jnp.float32)


def dot_nn(a, b):
    return jnp.dot(a, b, preferred_element_type=jnp.float32)


def silu(x):
    return x * jax.nn.sigmoid(x)


def split_bf16(x):
    high = x.astype(jnp.bfloat16)
    return high, (x - high.astype(jnp.float32)).astype(jnp.bfloat16)


def sweep_kernel(q_ref, f_ref, v_ref, slack_ref, spike_ref, local_ref, reach_ref, state_ref):
    head = pl.program_id(0)
    rows, width = q_ref.shape
    query = silu(q_ref[...].astype(jnp.float32)) * (width ** -0.5)
    value = v_ref[...]
    spikes = spike_ref[...]
    lane = lax.broadcasted_iota(jnp.int32, spikes.shape, 1)
    spike = jnp.sum(jnp.where(lane == head, spikes, 0.0), axis=1, keepdims=True)
    slack = slack_ref[...]
    down = lax.broadcasted_iota(jnp.int32, (rows, rows), 0)
    across = lax.broadcasted_iota(jnp.int32, (rows, rows), 1)
    scores = None
    for way in (0, 1):
        mask = (down >= across) if way == 0 else (down <= across)
        tri = jnp.where(mask, 1.0, 0.0).astype(jnp.bfloat16)
        key = slack * jax.nn.sigmoid(-f_ref[way].astype(jnp.float32))
        decay = jnp.log1p(-key) + spike
        high, low = split_bf16(decay)
        running = dot_nn(tri, high) + dot_nn(tri, low)
        final = running[rows - 1 : rows] if way == 0 else running[0:1]
        query_scaled = (query * jnp.exp(running)).astype(jnp.bfloat16)
        key_scaled = (key * jnp.exp(-running)).astype(jnp.bfloat16)
        key_end = (key * jnp.exp(final - running)).astype(jnp.bfloat16)
        part = jnp.where(mask, dot_nt(query_scaled, key_scaled), 0.0)
        scores = part if scores is None else scores + part
        reach_ref[way] = query_scaled
        state_ref[way, 0, 0:width] = dot_tn(value, key_end).astype(jnp.bfloat16)
        total_high, total_low = split_bf16(jnp.exp(final))
        place = lax.broadcasted_iota(jnp.int32, (PAD_ROWS, width), 0)
        state_ref[way, 0, width : width + PAD_ROWS] = jnp.where(
            place == 0,
            total_high.astype(jnp.float32),
            jnp.where(place == 1, total_low.astype(jnp.float32), 0.0),
        ).astype(jnp.bfloat16)
    local_ref[...] = dot_nn(scores.astype(jnp.bfloat16), value)


def sweep(queries, forget_logits, values, slack, spike):
    rows, columns = queries.shape
    heads = spike.shape[1]
    width = columns // heads
    by_head = pl.BlockSpec((rows, width), lambda h: (0, h))
    return pl.pallas_call(
        sweep_kernel,
        grid=(heads,),
        in_specs=[
            by_head,
            pl.BlockSpec((2, rows, width), lambda h: (0, 0, h)),
            by_head,
            pl.BlockSpec((1, width), lambda h: (0, h)),
            pl.BlockSpec((rows, heads), lambda h: (0, 0)),
        ],
        out_specs=[
            by_head,
            pl.BlockSpec((2, rows, width), lambda h: (0, 0, h)),
            pl.BlockSpec((2, 1, width + PAD_ROWS, width), lambda h: (0, h, 0, 0)),
        ],
        out_shape=[
            jax.ShapeDtypeStruct((rows, columns), jnp.float32),
            jax.ShapeDtypeStruct((2, rows, columns), jnp.bfloat16),
            jax.ShapeDtypeStruct((2, heads, width + PAD_ROWS, width), jnp.bfloat16),
        ],
        cost_estimate=pl.CostEstimate(
            flops=20 * rows * width * columns, bytes_accessed=8 * rows * columns, transcendentals=8 * rows * columns
        ),
        name="sweep",
    )(queries, forget_logits, values, slack.reshape(1, columns), spike)


def greet(axis, others, count):
    barrier = pltpu.get_barrier_semaphore()

    def signal(k, carry):
        pl.semaphore_signal(barrier, inc=1, device_id={axis: others(k)}, device_id_type=MESH)
        return carry

    lax.fori_loop(1, count, signal, 0)
    pl.semaphore_wait(barrier, count - 1)


def exchange_kernel(n, state_ref, enter_ref, held, made, out_sem, in_sem, out_sem2, in_sem2):
    me = lax.axis_index("sp")
    rows = enter_ref.shape[1]

    def other(k):
        return lax.rem(me + k, n)

    greet("sp", other, n)

    def first(k):
        there = other(k)
        return pltpu.make_async_remote_copy(
            src_ref=state_ref.at[there],
            dst_ref=held.at[me],
            send_sem=out_sem.at[k],
            recv_sem=in_sem.at[k],
            device_id={"sp": there},
            device_id_type=MESH,
        )

    def second(k):
        there = other(k)
        return pltpu.make_async_remote_copy(
            src_ref=made.at[there],
            dst_ref=enter_ref.at[me],
            send_sem=out_sem2.at[k],
            recv_sem=in_sem2.at[k],
            device_id={"sp": there},
            device_id_type=MESH,
        )

    def go(copy):
        def start(k, carry):
            copy(k).start()
            return carry

        lax.fori_loop(1, n, start, 0)

    def end(copy):
        def wait(k, carry):
            copy(k).wait()
            return carry

        lax.fori_loop(1, n, wait, 0)

    go(first)
    held[me] = state_ref[me]
    end(first)
    backward = me // (n // 2)

    def step(i, total):
        source = i + backward * (n - 1 - 2 * i)
        made[source] = total.astype(jnp.bfloat16)
        block = held[source].astype(jnp.float32)
        factor = block[rows : rows + 1] + block[rows + 1 : rows + 2]
        return factor * total + block[:rows]

    lax.fori_loop(0, n, step, jnp.zeros(enter_ref.shape[1:], jnp.float32))
    go(second)
    enter_ref[me] = made[me]
    end(second)


def exchange(states):
    n = lax.axis_size("sp")
    ways, heads, padded, width = states.shape
    depth = padded - PAD_ROWS
    cuts = n // (ways * heads)
    rows = depth // cuts
    if cuts > 1:
        body = states[:, :, :depth].reshape(ways, heads, cuts, rows, width)
        tail = jnp.broadcast_to(
            states[:, :, None, depth:], (ways, heads, cuts, PAD_ROWS, width)
        )
        states = jnp.concatenate([body, tail], axis=3)
    entered = pl.pallas_call(
        functools.partial(exchange_kernel, n),
        in_specs=[pl.BlockSpec(memory_space=pltpu.VMEM)],
        out_specs=pl.BlockSpec(memory_space=pltpu.VMEM),
        out_shape=jax.ShapeDtypeStruct((n, rows, width), jnp.bfloat16),
        scratch_shapes=[
            pltpu.VMEM((n, rows + PAD_ROWS, width), jnp.bfloat16),
            pltpu.VMEM((n, rows, width), jnp.bfloat16),
            pltpu.SemaphoreType.DMA((n,)),
            pltpu.SemaphoreType.DMA((n,)),
            pltpu.SemaphoreType.DMA((n,)),
            pltpu.SemaphoreType.DMA((n,)),
        ],
        compiler_params=pltpu.CompilerParams(collective_id=1, has_side_effects=True),
        name="exchange",
    )(states.reshape(n, rows + PAD_ROWS, width))
    return entered.reshape(ways, heads, depth, width)


def reshard_kernel(g, *refs):
    count = (len(refs) - 3) // 2
    gives, takes = refs[:count], refs[count : 2 * count]
    out_sem, in_sem, own_sem = refs[2 * count :]
    me = lax.axis_index("sp")
    base = me // g * g
    seat = me - base

    def other(k):
        return lax.rem(seat + k, g)

    greet("sp", lambda k: base + other(k), g)
    copies = []
    for k in range(1, g):
        there = other(k)
        for i in range(count):
            copies.append(
                pltpu.make_async_remote_copy(
                    src_ref=gives[i].at[there],
                    dst_ref=takes[i].at[seat],
                    send_sem=out_sem.at[i, k],
                    recv_sem=in_sem.at[i, k],
                    device_id={"sp": base + there},
                    device_id_type=MESH,
                )
            )
            copies[-1].start()
    for i in range(count):
        copies.append(pltpu.make_async_copy(gives[i].at[seat], takes[i].at[seat], own_sem.at[i]))
        copies[-1].start()
    for copy in copies:
        copy.wait()


def reshard(arrays, g, collective_id):
    count = len(arrays)
    return pl.pallas_call(
        functools.partial(reshard_kernel, g),
        in_specs=[pl.BlockSpec(memory_space=pltpu.VMEM)] * count,
        out_specs=[pl.BlockSpec(memory_space=pltpu.VMEM)] * count,
        out_shape=[jax.ShapeDtypeStruct(a.shape, a.dtype) for a in arrays],
        scratch_shapes=[
            pltpu.SemaphoreType.DMA((count, g)),
            pltpu.SemaphoreType.DMA((count, g)),
            pltpu.SemaphoreType.DMA((count,)),
        ],
        compiler_params=pltpu.CompilerParams(
            collective_id=collective_id, has_side_effects=True
        ),
        name="reshard",
    )(*arrays)


def gather_kernel(g, give, take, out_sem, in_sem):
    me = lax.axis_index("sp")
    base = me // g * g
    seat = me - base

    def other(k):
        return lax.rem(seat + k, g)

    greet("sp", lambda k: base + other(k), g)
    copies = []
    for k in range(1, g):
        copies.append(
            pltpu.make_async_remote_copy(
                src_ref=give,
                dst_ref=take.at[seat],
                send_sem=out_sem.at[k],
                recv_sem=in_sem.at[k],
                device_id={"sp": base + other(k)},
                device_id_type=MESH,
            )
        )
        copies[-1].start()
    take[seat] = give[...]
    for copy in copies:
        copy.wait()


def gather(array, g, collective_id):
    return pl.pallas_call(
        functools.partial(gather_kernel, g),
        in_specs=[pl.BlockSpec(memory_space=pltpu.VMEM)],
        out_specs=pl.BlockSpec(memory_space=pltpu.VMEM),
        out_shape=jax.ShapeDtypeStruct((g,) + array.shape, array.dtype),
        scratch_shapes=[pltpu.SemaphoreType.DMA((g,)), pltpu.SemaphoreType.DMA((g,))],
        compiler_params=pltpu.CompilerParams(
            collective_id=collective_id, has_side_effects=True
        ),
        name="gather",
    )(array).reshape((g * array.shape[0],) + array.shape[1:])


def project_kernel(local_ref, reach_ref, enter_ref, gain_ref, gate_ref, weight_ref, out_ref, total):
    head = pl.program_id(0)
    mix = (
        local_ref[...]
        + dot_nt(reach_ref[0], enter_ref[0, 0])
        + dot_nt(reach_ref[1], enter_ref[1, 0])
    )
    scale = lax.rsqrt(jnp.mean(mix * mix, axis=-1, keepdims=True) + NORM_EPS)
    gate = silu(gate_ref[...].astype(jnp.float32))
    mixed = (mix * scale * gain_ref[...].astype(jnp.float32) * gate).astype(jnp.bfloat16)
    term = dot_nn(mixed, weight_ref[...])

    @pl.when(head == 0)
    def _():
        total[...] = term

    @pl.when(head > 0)
    def _():
        total[...] += term

    @pl.when(head == pl.num_programs(0) - 1)
    def _():
        out_ref[...] = total[...].astype(jnp.bfloat16)


def project(local, reach, entered, gain, gate_logits, weight):
    rows, columns = local.shape
    heads, width = entered.shape[1], entered.shape[3]
    model = weight.shape[1]
    by_head = pl.BlockSpec((rows, width), lambda h: (0, h))
    return pl.pallas_call(
        project_kernel,
        grid=(heads,),
        in_specs=[
            by_head,
            pl.BlockSpec((2, rows, width), lambda h: (0, 0, h)),
            pl.BlockSpec((2, 1, width, width), lambda h: (0, h, 0, 0)),
            pl.BlockSpec((1, width), lambda h: (0, 0)),
            by_head,
            pl.BlockSpec((width, model), lambda h: (h, 0)),
        ],
        out_specs=pl.BlockSpec((rows, model), lambda h: (0, 0)),
        out_shape=jax.ShapeDtypeStruct((rows, model), jnp.bfloat16),
        scratch_shapes=[pltpu.VMEM((rows, model), jnp.float32)],
        cost_estimate=pl.CostEstimate(
            flops=2 * rows * columns * model, bytes_accessed=2 * columns * model, transcendentals=rows * columns
        ),
        name="project",
    )(local, reach, entered, gain.reshape(1, width), gate_logits, weight)


CORES = 2
PLANE = 4


def flip(i, k):
    out, bit = i, 1
    while bit <= k:
        if k & bit:
            out = out + bit - 2 * bit * (lax.rem(i // bit, 2))
        bit *= 2
    return out


def layer_kernel(
    nz,
    q_hbm, f_hbm, v_hbm, og_hbm, res_hbm, slack_ref, spike_ref, hgain_ref, mgain_ref, wo_hbm, gate_hbm, up_hbm, down_hbm,
    out_ref,
    q_v, f_v, v_v, og_v, res_v, wo_v, w_v,
    reach, scaled, locals_, gates, states, mate, chip, held, total, totals_in, entry, made, enter, beside, mixed, tok, inner,
    parts, terms,
    in_sem, w0_sem, w1_out, w1_in, x_out, x_in, y_out, y_in, d_out, d_in, p_out, p_in,
    s0_out, s0_in, s1_out, s1_in, s2_out, s2_in, s3_out, s3_in, s4_out, s4_in,
    up_out, up_in, dn_out, dn_in, r_out, r_in,
):
    rows, columns = q_v.shape
    width = hgain_ref.shape[1]
    heads = columns // width
    depth = gate_hbm.shape[0]
    units = w_v.shape[2]
    side = PLANE * CORES
    per = heads // PLANE
    me = lax.axis_index("sp")
    z, seat = me // side, lax.rem(me, side)
    q, c = seat // CORES, lax.rem(seat, CORES)

    def at(zz, qq, cc):
        return zz * side + qq * CORES + cc

    def copy(src, dst, out_sem, got_sem, there):
        return pltpu.make_async_remote_copy(
            src_ref=src, dst_ref=dst, send_sem=out_sem, recv_sem=got_sem,
            device_id={"sp": there}, device_id_type=MESH,
        )

    def when(condition, act):
        pl.when(condition)(act)

    zs = [z] + [flip(z, k) for k in range(1, nz)]
    qs = [q] + [flip(q, k) for k in range(1, PLANE)]
    along = [at(zz, q, c) for zz in zs]
    x_dev, y_dev, p_dev = at(z, qs[1], c), at(z, qs[2], c), at(z, q, 1 - c)
    up_dev, dn_dev = me + side, me - side

    loads = [
        pltpu.make_async_copy(src, dst, in_sem.at[i])
        for i, (src, dst) in enumerate(
            ((f_hbm, f_v), (q_hbm, q_v), (v_hbm, v_v), (og_hbm, og_v), (res_hbm, res_v), (wo_hbm, wo_v))
        )
    ]
    weights = (gate_hbm, up_hbm, down_hbm)

    def cut(a, zz):
        return weights[a].at[:, pl.ds(pl.multiple_of(zz * units, 128), units)]

    def strip(a, device):
        return w_v.at[a, pl.ds(pl.multiple_of(device * depth, depth), depth), :]

    own = [pltpu.make_async_copy(cut(a, z), strip(a, me), w0_sem.at[a]) for a in range(3)]
    for load in loads[:3]:
        load.start()
    for load in own:
        load.start()

    barrier = pltpu.get_barrier_semaphore()
    for k in range(1, nz):
        pl.semaphore_signal(barrier, inc=1, device_id={"sp": along[k]}, device_id_type=MESH)
    for k in range(1, side):
        pl.semaphore_signal(
            barrier, inc=1, device_id={"sp": z * side + lax.rem(seat + k, side)}, device_id_type=MESH
        )
    pl.semaphore_wait(barrier, nz - 1 + side - 1)

    members = ((0, 1), (2,))

    outer = jnp.logical_or(z == 0, z == nz - 1)
    order = (zs[0], zs[1], zs[3], zs[2])

    def source(part, k):
        return order[k] if part == 0 else k

    def first(part, k):
        return [
            copy(cut(a, zs[k]), strip(a, me), w1_out.at[0], w1_in.at[a, z], along[k]) for a in members[part]
        ]

    def first_start(*which):
        for part, k in which:
            for one in first(part, k):
                one.start()

    def first_wait(part, k):
        origin = source(part, k)

        @pl.when(origin != z)
        def _():
            for a in members[part]:
                copy(cut(a, z), strip(a, me), w1_out.at[0], w1_in.at[a, origin], along[1]).wait_recv()

    def piece(part, k, j):
        row = pl.multiple_of(at(source(part, k), qs[j], c) * depth, depth)
        lo, count = members[part][0], len(members[part])
        return w_v.at[pl.ds(lo, count), pl.ds(row, depth), :]

    def across_x(part, k):
        src = piece(part, k, 0)
        return copy(src, src, x_out.at[0], x_in.at[part, k], x_dev)

    def across_y(part, k):
        src = piece(part, k, 0)
        return copy(src, src, y_out.at[0], y_in.at[part, k], y_dev)

    def corner(part, k):
        near, there = (1, y_dev) if k < nz // 2 else (2, x_dev)
        src = piece(part, k, near)
        return copy(src, src, d_out.at[0], d_in.at[part, k], there)

    def partner(part, k, j):
        src = piece(part, k, j)
        return copy(src, src, p_out.at[0], p_in.at[part, k, j], p_dev)

    def spread(part, k):
        if part == 0 and k == 0:
            for a in members[0]:
                own[a].wait()
        else:
            first_wait(part, k)
        across_x(part, k).start()
        across_y(part, k).start()
        partner(part, k, 0).start()

    def onward(part, k):
        across_x(part, k).wait_recv()
        if k < nz // 2:
            corner(part, k).start()
        partner(part, k, 1).start()
        across_y(part, k).wait_recv()
        if k >= nz // 2:
            corner(part, k).start()
        partner(part, k, 2).start()

    def last(part, k):
        corner(part, k).wait_recv()
        partner(part, k, 3).start()

    def settle(part, k):
        for j in range(PLANE):
            partner(part, k, j).wait_recv()

    first_start((0, 1), (0, 3))
    spread(0, 0)
    for load in loads[3:]:
        load.start()

    down = lax.broadcasted_iota(jnp.int32, (rows, rows), 0)
    sideways = lax.broadcasted_iota(jnp.int32, (rows, rows), 1)
    masks = (down >= sideways, down <= sideways)
    for load in loads[:3]:
        load.wait()
    spikes = jnp.transpose(spike_ref[...])
    lane = lax.broadcasted_iota(jnp.int32, spikes.shape, 1)
    place = lax.broadcasted_iota(jnp.int32, (PAD_ROWS, width), 0)

    def pad(decay):
        high, low = split_bf16(decay)
        return jnp.where(
            place == 0, high.astype(jnp.float32), jnp.where(place == 1, low.astype(jnp.float32), 0.0)
        ).astype(jnp.bfloat16)

    def unpack(block):
        block = block.astype(jnp.float32)
        return block[:, width : width + 1] + block[:, width + 1 : width + 2], block[:, :width]

    def by_head(head):
        return pl.ds(pl.multiple_of(head * width, width), width)

    def make_states(group):
        def step(i, carry):
            head = group * per + i
            lanes = by_head(head)
            query = silu(q_v[:, lanes].astype(jnp.float32)) * (width ** -0.5)
            value = v_v[:, lanes]
            spike = jnp.sum(jnp.where(lane == head, spikes, 0.0), axis=1, keepdims=True)
            slack = slack_ref[:, lanes]
            for way in (0, 1):
                tri = jnp.where(masks[way], 1.0, 0.0).astype(jnp.bfloat16)
                key = slack * jax.nn.sigmoid(-f_v[way, :, lanes].astype(jnp.float32))
                decay = jnp.log(1.0 - key) + spike
                high, low = split_bf16(decay)
                running = dot_nn(tri, high) + dot_nn(tri, low)
                final = running[rows - 1 : rows] if way == 0 else running[0:1]
                reach[way, :, lanes] = (query * jnp.exp(running)).astype(jnp.bfloat16)
                key = key * jnp.exp(-running)
                scaled[way, :, lanes] = key.astype(jnp.bfloat16)
                final = jnp.exp(final)
                key_end = (key * final).astype(jnp.bfloat16)
                states[way, group, i, 0:width] = dot_tn(value, key_end).astype(jnp.bfloat16)
                states[way, group, i, width : width + PAD_ROWS] = pad(final)
            return carry

        lax.fori_loop(0, per, step, 0, unroll=True)

    def mate_copy(group):
        return copy(states.at[1 - c, group], mate.at[group], s0_out.at[group], s0_in.at[group], p_dev)

    def chip_copy(group):
        return copy(chip.at[group], held.at[q], s1_out.at[group], s1_in.at[q], at(z, group, c))

    def chip_arrival(group):
        return copy(chip.at[group], held.at[group], s1_out.at[group], s1_in.at[group], at(z, group, c))

    def join(group):
        mate_copy(group).wait_recv()
        factor, state = unpack(states[c, group])
        mate_factor, mate_state = unpack(mate[group])
        chip[group, :, 0:width] = (mate_factor * state + mate_state).astype(jnp.bfloat16)
        both = factor * mate_factor
        for i in range(per):
            chip[group, i, width : width + PAD_ROWS] = pad(both[i])
        when(q != group, lambda: chip_copy(group).start())

        @pl.when(q == group)
        def _():
            held[group] = chip[group]

    def local_step(head, carry):
        lanes = by_head(head)
        scores = None
        for way in (0, 1):
            part = jnp.where(masks[way], dot_nt(reach[way, :, lanes], scaled[way, :, lanes]), 0.0)
            scores = part if scores is None else scores + part
        locals_[:, lanes] = dot_nn(scores.astype(jnp.bfloat16), v_v[:, lanes])
        return carry

    for group in range(PLANE):
        make_states(group)
        mate_copy(group).start()
        if group > 0:
            join(group - 1)
    lax.fori_loop(0, heads // 2, local_step, 0, unroll=4)
    join(PLANE - 1)
    onward(0, 0)
    spread(0, 1)
    lax.fori_loop(heads // 2, heads, local_step, 0, unroll=4)

    for w in range(PLANE):
        when(w != q, lambda w=w: chip_arrival(w).wait_recv())

    def turn(i, count):
        return i + c * (count - 1 - 2 * i)

    entry[...] = jnp.zeros_like(entry)
    decay = jnp.ones((per, 1, width), jnp.float32)
    for i in range(PLANE):
        factor, state = unpack(held[turn(i, PLANE)])
        entry[...] = factor * entry[...] + state
        decay = factor * decay
    total[:, 0:width] = entry[...].astype(jnp.bfloat16)
    for i in range(per):
        total[i, width : width + PAD_ROWS] = pad(decay[i])

    def give_after(k):
        return (zs[k] > z) == (c == 0)

    def total_copy(k):
        return copy(total, totals_in.at[z], s2_out.at[k], s2_in.at[k], along[k])

    for k in range(nz - 1, 0, -1):
        when(give_after(k), lambda k=k: total_copy(k).start())
    own[2].wait()
    when(jnp.logical_not(outer), lambda: first_start((0, 2), (1, 1), (1, 3), (1, 2)))
    loads[3].wait()

    def gate_step(head, carry):
        lanes = by_head(head)
        gates[:, lanes] = silu(og_v[:, lanes].astype(jnp.float32)) * hgain_ref[...].astype(jnp.float32)
        return carry

    lax.fori_loop(0, heads, gate_step, 0)
    entry[...] = jnp.zeros_like(entry)
    for k in range(1, nz):
        when(jnp.logical_not(give_after(k)), lambda k=k: total_copy(k).wait_recv())
    for i in range(nz):
        origin = turn(i, nz)

        @pl.when(jnp.logical_and(origin != z, (origin < z) == (c == 0)))
        def _(origin=origin):
            factor, state = unpack(totals_in[origin])
            entry[...] = factor * entry[...] + state

    def enter_copy(w):
        return copy(made.at[w], enter.at[c, q], s3_out.at[w], s3_in.at[q], at(z, w, c))

    def enter_arrival(w):
        return copy(made.at[w], enter.at[c, w], s3_out.at[w], s3_in.at[w], at(z, w, c))

    def beside_copy(group):
        return copy(beside.at[group], enter.at[c, group], s4_out.at[group], s4_in.at[group], p_dev)

    def beside_arrival(group):
        return copy(beside.at[group], enter.at[1 - c, group], s4_out.at[group], s4_in.at[group], p_dev)

    for i in range(PLANE):
        origin = turn(i, PLANE)
        made[origin] = entry[...].astype(jnp.bfloat16)
        when(origin != q, lambda origin=origin: enter_copy(origin).start())
        factor, state = unpack(held[origin])
        entry[...] = factor * entry[...] + state
    enter[c, q] = made[q]
    when(outer, lambda: first_start((0, 2)))
    onward(0, 1)
    last(0, 0)
    spread(0, 2)
    for w in range(PLANE):
        when(w != q, lambda w=w: enter_arrival(w).wait_recv())
        factor, state = unpack(states[c, w])
        beside[w] = (factor * enter[c, w].astype(jnp.float32) + state).astype(jnp.bfloat16)
        beside_copy(w).start()
    for load in loads[4:]:
        load.wait()
    for w in range(PLANE):
        beside_arrival(w).wait_recv()

    when(outer, lambda: first_start((1, 2), (1, 3), (1, 1)))

    def mix_step(head, carry):
        lanes = by_head(head)
        group, i = head // per, lax.rem(head, per)
        mix = (
            locals_[:, lanes]
            + dot_nt(reach[0, :, lanes], enter[0, group, i])
            + dot_nt(reach[1, :, lanes], enter[1, group, i])
        )
        scale = lax.rsqrt(jnp.mean(mix * mix, axis=-1, keepdims=True) + NORM_EPS)
        mixed[:, lanes] = (mix * scale * gates[:, lanes]).astype(jnp.bfloat16)
        return carry

    lax.fori_loop(0, heads, mix_step, 0, unroll=4)
    chunk = columns // nz

    def hidden_step(i, carry):
        lanes = pl.ds(pl.multiple_of(i * chunk, chunk), chunk)
        part = dot_nn(mixed[...], wo_v[:, lanes]).astype(jnp.bfloat16).astype(jnp.float32)
        hidden = (res_v[:, lanes].astype(jnp.float32) + part).astype(jnp.bfloat16)
        res_v[:, lanes] = hidden
        hidden = hidden.astype(jnp.float32)
        return carry + jnp.sum(hidden * hidden, axis=-1, keepdims=True)

    squares = lax.fori_loop(0, columns // chunk, hidden_step, jnp.zeros((rows, 1), jnp.float32))
    scale = lax.rsqrt(squares / columns + NORM_EPS)
    for i in range(columns // width):
        lanes = pl.ds(i * width, width)
        gain = mgain_ref[i : i + 1].astype(jnp.float32)
        tok[z, :, lanes] = (res_v[:, lanes].astype(jnp.float32) * scale * gain).astype(jnp.bfloat16)

    def half(zz, h):
        return tok.at[zz, :, pl.ds(h * (columns // 2), columns // 2)]

    def up(zz, h):
        return copy(half(zz, h), half(zz, h), up_out.at[zz, h], up_in.at[zz, h], up_dev)

    def dn(zz, h):
        return copy(half(zz, h), half(zz, h), dn_out.at[zz, h], dn_in.at[zz, h], dn_dev)

    for h in (0, 1):
        when(z < nz - 1, lambda h=h: up(z, h).start())
        when(z > 0, lambda h=h: dn(z, h).start())

    def relay(k, h):
        @pl.when(z - k >= 0)
        def _():
            up(z - k, h).wait_recv()
            when(z < nz - 1, lambda: up(z - k, h).start())

        @pl.when(z + k < nz)
        def _():
            dn(z + k, h).wait_recv()
            when(z > 0, lambda: dn(z + k, h).start())

    def expand(zz):
        block = tok[zz]
        gate_act = dot_nn(block, w_v[0])
        up_act = dot_nn(block, w_v[1])
        inner[zz] = (silu(gate_act) * up_act).astype(jnp.bfloat16)

    def ordered(i):
        reach_dn, reach_up = z, nz - 1 - z
        near = jnp.minimum(reach_dn, reach_up)
        pair = (i + 1) // 2
        odd = lax.rem(i, 2)
        both = z + jnp.where(odd == 1, -pair, pair)
        single = jnp.where(reach_dn < reach_up, i, nz - 1 - i)
        return jnp.where(pair <= near, both, single)

    def lanes_of(s):
        return pl.ds(s * chunk, chunk)

    def lower(zz, s):
        out = dot_nt(inner[zz], w_v[2, s * chunk : (s + 1) * chunk])
        parts[zz, :, lanes_of(s)] = out.astype(jnp.bfloat16)

    def sum_up(zz, s):
        return copy(
            parts.at[zz, :, lanes_of(s)], terms.at[0, zz, :, lanes_of(s)], r_out.at[0], r_in.at[0, zz, s], up_dev
        )

    def sum_dn(zz, s):
        return copy(
            parts.at[zz, :, lanes_of(s)], terms.at[1, zz, :, lanes_of(s)], r_out.at[0], r_in.at[1, zz, s], dn_dev
        )

    def take(way, zz, s):
        (sum_up, sum_dn)[way](zz, s).wait_recv()
        parts[zz, :, lanes_of(s)] = (
            parts[zz, :, lanes_of(s)].astype(jnp.float32) + terms[way, zz, :, lanes_of(s)].astype(jnp.float32)
        ).astype(jnp.bfloat16)

    def ends(s, *far):
        for d in far:
            when(z == 0, lambda d=d: sum_up(d, s).start())
            when(z == nz - 1, lambda d=d: sum_dn(nz - 1 - d, s).start())

    def pass_up(at_z, zz, s):
        @pl.when(z == at_z)
        def _():
            take(0, zz, s)
            sum_up(zz, s).start()

    def pass_dn(at_z, zz, s):
        @pl.when(z == at_z)
        def _():
            take(1, zz, s)
            sum_dn(zz, s).start()

    def near_pass(s):
        pass_up(1, 2, s)
        pass_dn(2, 1, s)

    def far_pass(s):
        pass_up(1, 3, s)
        pass_dn(2, 0, s)

    def end_pass(s):
        pass_up(2, 3, s)
        pass_dn(1, 0, s)

    def work(lo, hi, act):
        def step(i, carry):
            act(ordered(i))
            return carry

        lax.fori_loop(lo, hi, step, 0)

    spread(0, 3)
    onward(0, 2)
    last(0, 1)
    onward(0, 3)
    spread(1, 0)
    spread(1, 1)
    relay(1, 0)
    last(0, 2)
    settle(0, 0)
    settle(0, 1)
    last(0, 3)
    onward(1, 0)
    spread(1, 2)
    relay(1, 1)
    settle(0, 2)
    settle(0, 3)
    work(1, 2, expand)
    onward(1, 1)
    spread(1, 3)
    relay(2, 0)
    last(1, 0)
    settle(1, 0)
    work(1, 2, lambda zz: lower(zz, 0))
    ends(0, 1)
    relay(2, 1)
    work(2, 3, expand)
    work(2, 3, lambda zz: lower(zz, 0))
    ends(0, 2)
    onward(1, 2)
    last(1, 1)
    settle(1, 1)
    work(1, 3, lambda zz: lower(zz, 1))
    ends(1, 2, 1)
    onward(1, 3)
    last(1, 2)
    settle(1, 2)
    near_pass(0)
    relay(3, 0)
    relay(3, 1)
    work(3, 4, expand)
    for s in range(3):
        work(3, 4, lambda zz, s=s: lower(zz, s))
        ends(s, 3)
    work(1, 3, lambda zz: lower(zz, 2))
    near_pass(1)
    last(1, 3)
    settle(1, 3)
    work(3, 4, lambda zz: lower(zz, 3))
    ends(3, 3)
    ends(2, 2, 1)
    work(1, 3, lambda zz: lower(zz, 3))
    ends(3, 2, 1)
    far_pass(0)
    far_pass(1)
    end_pass(0)
    far_pass(2)
    end_pass(1)
    work(0, 1, expand)
    for s in range(nz):
        work(0, 1, lambda zz, s=s: lower(zz, s))
    far_pass(3)
    end_pass(2)
    near_pass(2)
    end_pass(3)
    near_pass(3)

    def result(s):
        return pltpu.make_async_copy(mixed.at[:, lanes_of(s)], out_ref.at[:, lanes_of(s)], in_sem.at[6 + s])

    def finish(s):
        when(z > 0, lambda: sum_up(z, s).wait_recv())
        when(z < nz - 1, lambda: sum_dn(z, s).wait_recv())
        lanes = lanes_of(s)
        added = res_v[:, lanes].astype(jnp.float32) + parts[z, :, lanes].astype(jnp.float32)
        added = added + jnp.where(z > 0, terms[0, z, :, lanes].astype(jnp.float32), 0.0)
        added = added + jnp.where(z < nz - 1, terms[1, z, :, lanes].astype(jnp.float32), 0.0)
        mixed[:, lanes] = added.astype(jnp.bfloat16)
        result(s).start()

    for s in range(nz):
        finish(s)

    for s in range(nz):
        result(s).wait()
    def sent(src, sem, got_sem, there):
        copy(src, src, sem, got_sem, there).wait_send()

    sent(w_v.at[:, 0 : (nz - 1) * depth], w1_out.at[0], w1_in.at[0, 0], x_dev)
    sent(w_v.at[:, 0 : nz * depth], x_out.at[0], x_in.at[0, 0], x_dev)
    sent(w_v.at[:, 0 : nz * depth], y_out.at[0], y_in.at[0, 0], y_dev)
    sent(w_v.at[:, 0 : nz * depth], d_out.at[0], d_in.at[0, 0], x_dev)
    sent(w_v.at[:, 0 : PLANE * nz * depth], p_out.at[0], p_in.at[0, 0, 0], p_dev)
    sent(parts.at[0 : nz - 1], r_out.at[0], r_in.at[0, 0, 0], x_dev)
    for k in range(1, nz):
        when(give_after(k), lambda k=k: total_copy(k).wait_send())
    for k in range(nz):
        for h in (0, 1):
            when(jnp.logical_and(z < nz - 1, k <= z), lambda k=k, h=h: up(k, h).wait_send())
            when(jnp.logical_and(z > 0, k >= z), lambda k=k, h=h: dn(k, h).wait_send())
    for w in range(PLANE):
        mate_copy(w).wait_send()
        beside_copy(w).wait_send()

        @pl.when(w != q)
        def _(w=w):
            chip_copy(w).wait_send()
            enter_copy(w).wait_send()


def layer(queries, forget_logits, values, gate_logits, slack, spike, head_gain, output_weight, residual, mixer_gain, gate, up, down):
    n = lax.axis_size("sp")
    nz = n // (PLANE * CORES)
    rows, columns = queries.shape
    heads, width = spike.shape[1], head_gain.shape[0]
    depth, units = gate.shape[0], gate.shape[1] // nz
    per = heads // PLANE
    bf16, f32 = jnp.bfloat16, jnp.float32
    anywhere = pl.BlockSpec(memory_space=pl.ANY)
    near = pl.BlockSpec(memory_space=pltpu.VMEM)
    dma = pltpu.SemaphoreType.DMA
    padded = width + PAD_ROWS

    def pairs(*shape):
        return [dma(shape), dma(shape)]

    def one_out(*shape):
        return [dma((1,)), dma(shape)]

    return pl.pallas_call(
        functools.partial(layer_kernel, nz),
        in_specs=[anywhere] * 5 + [near] * 4 + [anywhere] * 4,
        out_specs=anywhere,
        out_shape=jax.ShapeDtypeStruct((rows, columns), bf16),
        scratch_shapes=[
            pltpu.VMEM((rows, columns), bf16),
            pltpu.VMEM((2, rows, columns), bf16),
            pltpu.VMEM((rows, columns), bf16),
            pltpu.VMEM((rows, columns), bf16),
            pltpu.VMEM((rows, columns), bf16),
            pltpu.VMEM(output_weight.shape, bf16),
            pltpu.VMEM((3, n * depth, units), bf16),
            pltpu.VMEM((2, rows, columns), bf16),
            pltpu.VMEM((2, rows, columns), bf16),
            pltpu.VMEM((rows, columns), f32),
            pltpu.VMEM((rows, columns), f32),
            pltpu.VMEM((2, PLANE, per, padded, width), bf16),
            pltpu.VMEM((PLANE, per, padded, width), bf16),
            pltpu.VMEM((PLANE, per, padded, width), bf16),
            pltpu.VMEM((PLANE, per, padded, width), bf16),
            pltpu.VMEM((per, padded, width), bf16),
            pltpu.VMEM((nz, per, padded, width), bf16),
            pltpu.VMEM((per, width, width), f32),
            pltpu.VMEM((PLANE, per, width, width), bf16),
            pltpu.VMEM((2, PLANE, per, width, width), bf16),
            pltpu.VMEM((PLANE, per, width, width), bf16),
            pltpu.VMEM((rows, columns), bf16),
            pltpu.VMEM((nz, rows, columns), bf16),
            pltpu.VMEM((nz, rows, units), bf16),
            pltpu.VMEM((nz, rows, columns), bf16),
            pltpu.VMEM((2, nz, rows, columns), bf16),
            dma((6 + nz,)),
            dma((3,)),
            *one_out(3, nz),
            *one_out(2, nz),
            *one_out(2, nz),
            *one_out(2, nz),
            *one_out(2, nz, PLANE),
            *pairs(PLANE),
            *pairs(PLANE),
            *pairs(nz),
            *pairs(PLANE),
            *pairs(PLANE),
            *pairs(nz, 2),
            *pairs(nz, 2),
            *one_out(2, nz, nz),
        ],
        compiler_params=pltpu.CompilerParams(
            collective_id=7, has_side_effects=True, vmem_limit_bytes=60 * 1024 * 1024
        ),
        name="layer",
    )(
        queries, forget_logits, values, gate_logits, residual, slack.reshape(1, columns), spike.T,
        head_gain.reshape(1, width), mixer_gain.reshape(columns // width, width), output_weight, gate, up, down.T,
    )


def local(
    queries,
    forget_logits,
    value_matrix,
    output_gate_logits,
    forget_slack,
    spike_log_forget,
    head_norm_gain,
    output_weight,
    residual,
    mixer_norm_gain,
    mixer_gate_weight,
    mixer_up_weight,
    mixer_down_weight,
):
    n, tp = lax.axis_size("sp"), lax.axis_size("tp")
    nz, tail = n // (PLANE * CORES), n % (PLANE * CORES)
    if tp == 1 and tail == 0 and nz == PLANE and mixer_gate_weight.shape[1] % (128 * nz) == 0:
        return layer(
            queries,
            forget_logits,
            value_matrix,
            output_gate_logits,
            forget_slack,
            spike_log_forget,
            head_norm_gain,
            output_weight,
            residual,
            mixer_norm_gain,
            mixer_gate_weight,
            mixer_up_weight,
            mixer_down_weight,
        )
    g = GROUP
    row_count = queries.shape[0]
    depth, units = mixer_gate_weight.shape
    far = [[b * g + j for b in range(n // g)] for j in range(g)]

    def cut(weight):
        return weight.reshape(depth, g, units // g).transpose(1, 0, 2)

    pieces = reshard([cut(mixer_gate_weight), cut(mixer_up_weight), cut(mixer_down_weight.T)], g, 2)
    gate_weight, up_weight, down_weight = (
        lax.all_gather(
            p.reshape(g * depth, units // g), "sp", axis=0, tiled=True, axis_index_groups=far
        )
        for p in pieces
    )

    local_out, reach, states = sweep(
        queries, forget_logits, value_matrix, forget_slack, spike_log_forget
    )
    entered = exchange(states)
    part = project(local_out, reach, entered, head_norm_gain, output_gate_logits, output_weight)
    part_rows = row_count // tp
    if tp > 1:
        part = lax.psum_scatter(part, "tp", scatter_dimension=0, tiled=True)
        residual = lax.dynamic_slice_in_dim(
            residual, lax.axis_index("tp") * part_rows, part_rows, 0
        )
    hidden = (residual.astype(jnp.float32) + part.astype(jnp.float32)).astype(jnp.bfloat16)
    hidden_f = hidden.astype(jnp.float32)
    normed = (
        hidden_f
        * lax.rsqrt(jnp.mean(hidden_f * hidden_f, axis=-1, keepdims=True) + NORM_EPS)
        * mixer_norm_gain.astype(jnp.float32)
    ).astype(jnp.bfloat16)
    normed = gather(normed, g, 4)
    if tp > 1:
        normed = lax.all_gather(normed, "tp", axis=0, tiled=True)
    gate_act = dot_nn(normed, gate_weight)
    up_act = dot_nn(normed, up_weight)
    inner = (silu(gate_act) * up_act).astype(jnp.bfloat16)
    lowered = dot_nt(inner, down_weight).astype(jnp.bfloat16)
    if tp > 1:
        lowered = lax.psum_scatter(lowered, "tp", scatter_dimension=0, tiled=True)
    (terms,) = reshard([lowered.reshape(g, part_rows, lowered.shape[1])], g, 3)
    added = jnp.sum(terms.astype(jnp.float32), axis=0)
    return (hidden_f + added).astype(jnp.bfloat16)


def solution(mesh):
    placed = (
        P("sp", "tp"),
        P(None, "sp", "tp"),
        P("sp", "tp"),
        P("sp", "tp"),
        P("tp"),
        P("sp", "tp"),
        P(),
        P("tp", None),
        P("sp", None),
        P(),
        P("sp", "tp"),
        P("sp", "tp"),
        P("tp", "sp"),
    )
    return jax.shard_map(
        local, mesh=mesh, in_specs=placed, out_specs=P(("sp", "tp"), None), check_vma=False
    )
```

```python
import functools

import jax
import jax.numpy as jnp
from jax import lax
from jax.experimental import pallas as pl
from jax.experimental.pallas import tpu as pltpu
from jax.sharding import PartitionSpec as P

NORM_EPS = 1e-06
MESH = pl.DeviceIdType.MESH
PAD_ROWS = 16
GROUP = 8


def dot_nt(a, b):
    return lax.dot_general(a, b, (((1,), (1,)), ((), ())), preferred_element_type=jnp.float32)


def dot_tn(a, b):
    return lax.dot_general(a, b, (((0,), (0,)), ((), ())), preferred_element_type=jnp.float32)


def dot_nn(a, b):
    return jnp.dot(a, b, preferred_element_type=jnp.float32)


def silu(x):
    return x * jax.nn.sigmoid(x)


def split_bf16(x):
    high = x.astype(jnp.bfloat16)
    return high, (x - high.astype(jnp.float32)).astype(jnp.bfloat16)


def sweep_kernel(q_ref, f_ref, v_ref, slack_ref, spike_ref, local_ref, reach_ref, state_ref):
    head = pl.program_id(0)
    rows, width = q_ref.shape
    query = silu(q_ref[...].astype(jnp.float32)) * (width ** -0.5)
    value = v_ref[...]
    spikes = spike_ref[...]
    lane = lax.broadcasted_iota(jnp.int32, spikes.shape, 1)
    spike = jnp.sum(jnp.where(lane == head, spikes, 0.0), axis=1, keepdims=True)
    slack = slack_ref[...]
    down = lax.broadcasted_iota(jnp.int32, (rows, rows), 0)
    across = lax.broadcasted_iota(jnp.int32, (rows, rows), 1)
    scores = None
    for way in (0, 1):
        mask = (down >= across) if way == 0 else (down <= across)
        tri = jnp.where(mask, 1.0, 0.0).astype(jnp.bfloat16)
        key = slack * jax.nn.sigmoid(-f_ref[way].astype(jnp.float32))
        decay = jnp.log1p(-key) + spike
        high, low = split_bf16(decay)
        running = dot_nn(tri, high) + dot_nn(tri, low)
        final = running[rows - 1 : rows] if way == 0 else running[0:1]
        query_scaled = (query * jnp.exp(running)).astype(jnp.bfloat16)
        key_scaled = (key * jnp.exp(-running)).astype(jnp.bfloat16)
        key_end = (key * jnp.exp(final - running)).astype(jnp.bfloat16)
        part = jnp.where(mask, dot_nt(query_scaled, key_scaled), 0.0)
        scores = part if scores is None else scores + part
        reach_ref[way] = query_scaled
        state_ref[way, 0, 0:width] = dot_tn(value, key_end).astype(jnp.bfloat16)
        total_high, total_low = split_bf16(jnp.exp(final))
        place = lax.broadcasted_iota(jnp.int32, (PAD_ROWS, width), 0)
        state_ref[way, 0, width : width + PAD_ROWS] = jnp.where(
            place == 0,
            total_high.astype(jnp.float32),
            jnp.where(place == 1, total_low.astype(jnp.float32), 0.0),
        ).astype(jnp.bfloat16)
    local_ref[...] = dot_nn(scores.astype(jnp.bfloat16), value)


def sweep(queries, forget_logits, values, slack, spike):
    rows, columns = queries.shape
    heads = spike.shape[1]
    width = columns // heads
    by_head = pl.BlockSpec((rows, width), lambda h: (0, h))
    return pl.pallas_call(
        sweep_kernel,
        grid=(heads,),
        in_specs=[
            by_head,
            pl.BlockSpec((2, rows, width), lambda h: (0, 0, h)),
            by_head,
            pl.BlockSpec((1, width), lambda h: (0, h)),
            pl.BlockSpec((rows, heads), lambda h: (0, 0)),
        ],
        out_specs=[
            by_head,
            pl.BlockSpec((2, rows, width), lambda h: (0, 0, h)),
            pl.BlockSpec((2, 1, width + PAD_ROWS, width), lambda h: (0, h, 0, 0)),
        ],
        out_shape=[
            jax.ShapeDtypeStruct((rows, columns), jnp.float32),
            jax.ShapeDtypeStruct((2, rows, columns), jnp.bfloat16),
            jax.ShapeDtypeStruct((2, heads, width + PAD_ROWS, width), jnp.bfloat16),
        ],
        cost_estimate=pl.CostEstimate(
            flops=20 * rows * width * columns, bytes_accessed=8 * rows * columns, transcendentals=8 * rows * columns
        ),
        name="sweep",
    )(queries, forget_logits, values, slack.reshape(1, columns), spike)


def greet(axis, others, count):
    barrier = pltpu.get_barrier_semaphore()

    def signal(k, carry):
        pl.semaphore_signal(barrier, inc=1, device_id={axis: others(k)}, device_id_type=MESH)
        return carry

    lax.fori_loop(1, count, signal, 0)
    pl.semaphore_wait(barrier, count - 1)


def exchange_kernel(n, state_ref, enter_ref, held, made, out_sem, in_sem, out_sem2, in_sem2):
    me = lax.axis_index("sp")
    rows = enter_ref.shape[1]

    def other(k):
        return lax.rem(me + k, n)

    greet("sp", other, n)

    def first(k):
        there = other(k)
        return pltpu.make_async_remote_copy(
            src_ref=state_ref.at[there],
            dst_ref=held.at[me],
            send_sem=out_sem.at[k],
            recv_sem=in_sem.at[k],
            device_id={"sp": there},
            device_id_type=MESH,
        )

    def second(k):
        there = other(k)
        return pltpu.make_async_remote_copy(
            src_ref=made.at[there],
            dst_ref=enter_ref.at[me],
            send_sem=out_sem2.at[k],
            recv_sem=in_sem2.at[k],
            device_id={"sp": there},
            device_id_type=MESH,
        )

    def go(copy):
        def start(k, carry):
            copy(k).start()
            return carry

        lax.fori_loop(1, n, start, 0)

    def end(copy):
        def wait(k, carry):
            copy(k).wait()
            return carry

        lax.fori_loop(1, n, wait, 0)

    go(first)
    held[me] = state_ref[me]
    end(first)
    backward = me // (n // 2)

    def step(i, total):
        source = i + backward * (n - 1 - 2 * i)
        made[source] = total.astype(jnp.bfloat16)
        block = held[source].astype(jnp.float32)
        factor = block[rows : rows + 1] + block[rows + 1 : rows + 2]
        return factor * total + block[:rows]

    lax.fori_loop(0, n, step, jnp.zeros(enter_ref.shape[1:], jnp.float32))
    go(second)
    enter_ref[me] = made[me]
    end(second)


def exchange(states):
    n = lax.axis_size("sp")
    ways, heads, padded, width = states.shape
    depth = padded - PAD_ROWS
    cuts = n // (ways * heads)
    rows = depth // cuts
    if cuts > 1:
        body = states[:, :, :depth].reshape(ways, heads, cuts, rows, width)
        tail = jnp.broadcast_to(
            states[:, :, None, depth:], (ways, heads, cuts, PAD_ROWS, width)
        )
        states = jnp.concatenate([body, tail], axis=3)
    entered = pl.pallas_call(
        functools.partial(exchange_kernel, n),
        in_specs=[pl.BlockSpec(memory_space=pltpu.VMEM)],
        out_specs=pl.BlockSpec(memory_space=pltpu.VMEM),
        out_shape=jax.ShapeDtypeStruct((n, rows, width), jnp.bfloat16),
        scratch_shapes=[
            pltpu.VMEM((n, rows + PAD_ROWS, width), jnp.bfloat16),
            pltpu.VMEM((n, rows, width), jnp.bfloat16),
            pltpu.SemaphoreType.DMA((n,)),
            pltpu.SemaphoreType.DMA((n,)),
            pltpu.SemaphoreType.DMA((n,)),
            pltpu.SemaphoreType.DMA((n,)),
        ],
        compiler_params=pltpu.CompilerParams(collective_id=1, has_side_effects=True),
        name="exchange",
    )(states.reshape(n, rows + PAD_ROWS, width))
    return entered.reshape(ways, heads, depth, width)


def reshard_kernel(g, *refs):
    count = (len(refs) - 3) // 2
    gives, takes = refs[:count], refs[count : 2 * count]
    out_sem, in_sem, own_sem = refs[2 * count :]
    me = lax.axis_index("sp")
    base = me // g * g
    seat = me - base

    def other(k):
        return lax.rem(seat + k, g)

    greet("sp", lambda k: base + other(k), g)
    copies = []
    for k in range(1, g):
        there = other(k)
        for i in range(count):
            copies.append(
                pltpu.make_async_remote_copy(
                    src_ref=gives[i].at[there],
                    dst_ref=takes[i].at[seat],
                    send_sem=out_sem.at[i, k],
                    recv_sem=in_sem.at[i, k],
                    device_id={"sp": base + there},
                    device_id_type=MESH,
                )
            )
            copies[-1].start()
    for i in range(count):
        copies.append(pltpu.make_async_copy(gives[i].at[seat], takes[i].at[seat], own_sem.at[i]))
        copies[-1].start()
    for copy in copies:
        copy.wait()


def reshard(arrays, g, collective_id):
    count = len(arrays)
    return pl.pallas_call(
        functools.partial(reshard_kernel, g),
        in_specs=[pl.BlockSpec(memory_space=pltpu.VMEM)] * count,
        out_specs=[pl.BlockSpec(memory_space=pltpu.VMEM)] * count,
        out_shape=[jax.ShapeDtypeStruct(a.shape, a.dtype) for a in arrays],
        scratch_shapes=[
            pltpu.SemaphoreType.DMA((count, g)),
            pltpu.SemaphoreType.DMA((count, g)),
            pltpu.SemaphoreType.DMA((count,)),
        ],
        compiler_params=pltpu.CompilerParams(
            collective_id=collective_id, has_side_effects=True
        ),
        name="reshard",
    )(*arrays)


def gather_kernel(g, give, take, out_sem, in_sem):
    me = lax.axis_index("sp")
    base = me // g * g
    seat = me - base

    def other(k):
        return lax.rem(seat + k, g)

    greet("sp", lambda k: base + other(k), g)
    copies = []
    for k in range(1, g):
        copies.append(
            pltpu.make_async_remote_copy(
                src_ref=give,
                dst_ref=take.at[seat],
                send_sem=out_sem.at[k],
                recv_sem=in_sem.at[k],
                device_id={"sp": base + other(k)},
                device_id_type=MESH,
            )
        )
        copies[-1].start()
    take[seat] = give[...]
    for copy in copies:
        copy.wait()


def gather(array, g, collective_id):
    return pl.pallas_call(
        functools.partial(gather_kernel, g),
        in_specs=[pl.BlockSpec(memory_space=pltpu.VMEM)],
        out_specs=pl.BlockSpec(memory_space=pltpu.VMEM),
        out_shape=jax.ShapeDtypeStruct((g,) + array.shape, array.dtype),
        scratch_shapes=[pltpu.SemaphoreType.DMA((g,)), pltpu.SemaphoreType.DMA((g,))],
        compiler_params=pltpu.CompilerParams(
            collective_id=collective_id, has_side_effects=True
        ),
        name="gather",
    )(array).reshape((g * array.shape[0],) + array.shape[1:])


def project_kernel(local_ref, reach_ref, enter_ref, gain_ref, gate_ref, weight_ref, out_ref, total):
    head = pl.program_id(0)
    mix = (
        local_ref[...]
        + dot_nt(reach_ref[0], enter_ref[0, 0])
        + dot_nt(reach_ref[1], enter_ref[1, 0])
    )
    scale = lax.rsqrt(jnp.mean(mix * mix, axis=-1, keepdims=True) + NORM_EPS)
    gate = silu(gate_ref[...].astype(jnp.float32))
    mixed = (mix * scale * gain_ref[...].astype(jnp.float32) * gate).astype(jnp.bfloat16)
    term = dot_nn(mixed, weight_ref[...])

    @pl.when(head == 0)
    def _():
        total[...] = term

    @pl.when(head > 0)
    def _():
        total[...] += term

    @pl.when(head == pl.num_programs(0) - 1)
    def _():
        out_ref[...] = total[...].astype(jnp.bfloat16)


def project(local, reach, entered, gain, gate_logits, weight):
    rows, columns = local.shape
    heads, width = entered.shape[1], entered.shape[3]
    model = weight.shape[1]
    by_head = pl.BlockSpec((rows, width), lambda h: (0, h))
    return pl.pallas_call(
        project_kernel,
        grid=(heads,),
        in_specs=[
            by_head,
            pl.BlockSpec((2, rows, width), lambda h: (0, 0, h)),
            pl.BlockSpec((2, 1, width, width), lambda h: (0, h, 0, 0)),
            pl.BlockSpec((1, width), lambda h: (0, 0)),
            by_head,
            pl.BlockSpec((width, model), lambda h: (h, 0)),
        ],
        out_specs=pl.BlockSpec((rows, model), lambda h: (0, 0)),
        out_shape=jax.ShapeDtypeStruct((rows, model), jnp.bfloat16),
        scratch_shapes=[pltpu.VMEM((rows, model), jnp.float32)],
        cost_estimate=pl.CostEstimate(
            flops=2 * rows * columns * model, bytes_accessed=2 * columns * model, transcendentals=rows * columns
        ),
        name="project",
    )(local, reach, entered, gain.reshape(1, width), gate_logits, weight)


CORES = 2
PLANE = 4


def flip(i, k):
    out, bit = i, 1
    while bit <= k:
        if k & bit:
            out = out + bit - 2 * bit * (lax.rem(i // bit, 2))
        bit *= 2
    return out


def layer_kernel(
    nz,
    q_hbm, f_hbm, v_hbm, og_hbm, res_hbm, slack_ref, spike_ref, hgain_ref, mgain_ref, wo_hbm, gate_hbm, up_hbm, down_hbm,
    out_ref,
    q_v, f_v, v_v, og_v, res_v, wo_v, w_v,
    reach, scaled, locals_, gates, states, mate, chip, held, total, totals_in, entry, made, enter, beside, mixed, tok, inner,
    parts, terms,
    in_sem, w0_sem, w1_out, w1_in, x_out, x_in, y_out, y_in, d_out, d_in, p_out, p_in,
    s0_out, s0_in, s1_out, s1_in, s2_out, s2_in, s3_out, s3_in, s4_out, s4_in,
    up_out, up_in, dn_out, dn_in, r_out, r_in,
):
    rows, columns = q_v.shape
    width = hgain_ref.shape[1]
    heads = columns // width
    depth = gate_hbm.shape[0]
    units = w_v.shape[2]
    side = PLANE * CORES
    per = heads // PLANE
    me = lax.axis_index("sp")
    z, seat = me // side, lax.rem(me, side)
    q, c = seat // CORES, lax.rem(seat, CORES)

    def at(zz, qq, cc):
        return zz * side + qq * CORES + cc

    def copy(src, dst, out_sem, got_sem, there):
        return pltpu.make_async_remote_copy(
            src_ref=src, dst_ref=dst, send_sem=out_sem, recv_sem=got_sem,
            device_id={"sp": there}, device_id_type=MESH,
        )

    def when(condition, act):
        pl.when(condition)(act)

    zs = [z] + [flip(z, k) for k in range(1, nz)]
    qs = [q] + [flip(q, k) for k in range(1, PLANE)]
    along = [at(zz, q, c) for zz in zs]
    x_dev, y_dev, p_dev = at(z, qs[1], c), at(z, qs[2], c), at(z, q, 1 - c)
    up_dev, dn_dev = me + side, me - side

    loads = [
        pltpu.make_async_copy(src, dst, in_sem.at[i])
        for i, (src, dst) in enumerate(
            ((f_hbm, f_v), (q_hbm, q_v), (v_hbm, v_v), (og_hbm, og_v), (res_hbm, res_v), (wo_hbm, wo_v))
        )
    ]
    weights = (gate_hbm, up_hbm, down_hbm)

    def cut(a, zz):
        return weights[a].at[:, pl.ds(pl.multiple_of(zz * units, 128), units)]

    def strip(a, device):
        return w_v.at[a, pl.ds(pl.multiple_of(device * depth, depth), depth), :]

    own = [pltpu.make_async_copy(cut(a, z), strip(a, me), w0_sem.at[a]) for a in range(3)]
    for load in loads[:3]:
        load.start()
    for load in own:
        load.start()

    barrier = pltpu.get_barrier_semaphore()
    for k in range(1, nz):
        pl.semaphore_signal(barrier, inc=1, device_id={"sp": along[k]}, device_id_type=MESH)
    for k in range(1, side):
        pl.semaphore_signal(
            barrier, inc=1, device_id={"sp": z * side + lax.rem(seat + k, side)}, device_id_type=MESH
        )
    pl.semaphore_wait(barrier, nz - 1 + side - 1)

    members = ((0, 1), (2,))

    outer = jnp.logical_or(z == 0, z == nz - 1)
    order = (zs[0], zs[1], zs[3], zs[2])

    def source(part, k):
        return order[k] if part == 0 else k

    def first(part, k):
        return [
            copy(cut(a, zs[k]), strip(a, me), w1_out.at[0], w1_in.at[a, z], along[k]) for a in members[part]
        ]

    def first_start(*which):
        for part, k in which:
            for one in first(part, k):
                one.start()

    def first_wait(part, k):
        origin = source(part, k)

        @pl.when(origin != z)
        def _():
            for a in members[part]:
                copy(cut(a, z), strip(a, me), w1_out.at[0], w1_in.at[a, origin], along[1]).wait_recv()

    def piece(part, k, j):
        row = pl.multiple_of(at(source(part, k), qs[j], c) * depth, depth)
        lo, count = members[part][0], len(members[part])
        return w_v.at[pl.ds(lo, count), pl.ds(row, depth), :]

    def across_x(part, k):
        src = piece(part, k, 0)
        return copy(src, src, x_out.at[0], x_in.at[part, k], x_dev)

    def across_y(part, k):
        src = piece(part, k, 0)
        return copy(src, src, y_out.at[0], y_in.at[part, k], y_dev)

    def corner(part, k, j):
        near, there = ((1, y_dev), (2, x_dev))[j]
        row, lo, count = at(source(part, k), qs[near], c) * depth, j, depth
        if part == 1:
            row, lo, count = row + j * (depth // 2), 2, depth // 2
        src = w_v.at[pl.ds(lo, 1), pl.ds(pl.multiple_of(row, count), count), :]
        return copy(src, src, d_out.at[0], d_in.at[j, part, k], there)

    def partner(part, k, j):
        src = piece(part, k, j)
        return copy(src, src, p_out.at[0], p_in.at[part, k, j], p_dev)

    def spread(part, k):
        if part == 0 and k == 0:
            for a in members[0]:
                own[a].wait()
        else:
            first_wait(part, k)
        across_x(part, k).start()
        across_y(part, k).start()
        partner(part, k, 0).start()

    def onward(part, k):
        across_x(part, k).wait_recv()
        corner(part, k, 0).start()
        partner(part, k, 1).start()
        across_y(part, k).wait_recv()
        corner(part, k, 1).start()
        partner(part, k, 2).start()

    def last(part, k):
        corner(part, k, 0).wait_recv()
        corner(part, k, 1).wait_recv()
        partner(part, k, 3).start()

    def settle(part, k):
        for j in range(PLANE):
            partner(part, k, j).wait_recv()

    first_start((0, 1), (0, 3))
    spread(0, 0)
    for load in loads[3:]:
        load.start()

    down = lax.broadcasted_iota(jnp.int32, (rows, rows), 0)
    sideways = lax.broadcasted_iota(jnp.int32, (rows, rows), 1)
    masks = (down >= sideways, down <= sideways)
    for load in loads[:3]:
        load.wait()
    spikes = jnp.transpose(spike_ref[...])
    lane = lax.broadcasted_iota(jnp.int32, spikes.shape, 1)
    place = lax.broadcasted_iota(jnp.int32, (PAD_ROWS, width), 0)

    def pad(decay):
        high, low = split_bf16(decay)
        return jnp.where(
            place == 0, high.astype(jnp.float32), jnp.where(place == 1, low.astype(jnp.float32), 0.0)
        ).astype(jnp.bfloat16)

    def unpack(block):
        block = block.astype(jnp.float32)
        return block[:, width : width + 1] + block[:, width + 1 : width + 2], block[:, :width]

    def by_head(head):
        return pl.ds(pl.multiple_of(head * width, width), width)

    def make_states(group):
        def step(i, carry):
            head = group * per + i
            lanes = by_head(head)
            query = silu(q_v[:, lanes].astype(jnp.float32)) * (width ** -0.5)
            value = v_v[:, lanes]
            spike = jnp.sum(jnp.where(lane == head, spikes, 0.0), axis=1, keepdims=True)
            slack = slack_ref[:, lanes]
            for way in (0, 1):
                tri = jnp.where(masks[way], 1.0, 0.0).astype(jnp.bfloat16)
                key = slack * jax.nn.sigmoid(-f_v[way, :, lanes].astype(jnp.float32))
                decay = jnp.log(1.0 - key) + spike
                high, low = split_bf16(decay)
                running = dot_nn(tri, high) + dot_nn(tri, low)
                final = running[rows - 1 : rows] if way == 0 else running[0:1]
                reach[way, :, lanes] = (query * jnp.exp(running)).astype(jnp.bfloat16)
                key = key * jnp.exp(-running)
                scaled[way, :, lanes] = key.astype(jnp.bfloat16)
                final = jnp.exp(final)
                key_end = (key * final).astype(jnp.bfloat16)
                states[way, group, i, 0:width] = dot_tn(value, key_end).astype(jnp.bfloat16)
                states[way, group, i, width : width + PAD_ROWS] = pad(final)
            return carry

        lax.fori_loop(0, per, step, 0, unroll=True)

    def mate_copy(group):
        return copy(states.at[1 - c, group], mate.at[group], s0_out.at[group], s0_in.at[group], p_dev)

    def chip_copy(group):
        return copy(chip.at[group], held.at[q], s1_out.at[group], s1_in.at[q], at(z, group, c))

    def chip_arrival(group):
        return copy(chip.at[group], held.at[group], s1_out.at[group], s1_in.at[group], at(z, group, c))

    def join(group):
        mate_copy(group).wait_recv()
        factor, state = unpack(states[c, group])
        mate_factor, mate_state = unpack(mate[group])
        chip[group, :, 0:width] = (mate_factor * state + mate_state).astype(jnp.bfloat16)
        both = factor * mate_factor
        for i in range(per):
            chip[group, i, width : width + PAD_ROWS] = pad(both[i])
        when(q != group, lambda: chip_copy(group).start())

        @pl.when(q == group)
        def _():
            held[group] = chip[group]

    def local_step(head, carry):
        lanes = by_head(head)
        scores = None
        for way in (0, 1):
            part = jnp.where(masks[way], dot_nt(reach[way, :, lanes], scaled[way, :, lanes]), 0.0)
            scores = part if scores is None else scores + part
        locals_[:, lanes] = dot_nn(scores.astype(jnp.bfloat16), v_v[:, lanes])
        return carry

    for group in range(PLANE):
        make_states(group)
        mate_copy(group).start()
        if group > 0:
            join(group - 1)
    lax.fori_loop(0, heads // 2, local_step, 0, unroll=4)
    join(PLANE - 1)
    onward(0, 0)
    spread(0, 1)
    lax.fori_loop(heads // 2, heads, local_step, 0, unroll=4)

    for w in range(PLANE):
        when(w != q, lambda w=w: chip_arrival(w).wait_recv())

    def turn(i, count):
        return i + c * (count - 1 - 2 * i)

    entry[...] = jnp.zeros_like(entry)
    decay = jnp.ones((per, 1, width), jnp.float32)
    for i in range(PLANE):
        factor, state = unpack(held[turn(i, PLANE)])
        entry[...] = factor * entry[...] + state
        decay = factor * decay
    total[:, 0:width] = entry[...].astype(jnp.bfloat16)
    for i in range(per):
        total[i, width : width + PAD_ROWS] = pad(decay[i])

    def give_after(k):
        return (zs[k] > z) == (c == 0)

    def total_copy(k):
        return copy(total, totals_in.at[z], s2_out.at[k], s2_in.at[k], along[k])

    for k in range(nz - 1, 0, -1):
        when(give_after(k), lambda k=k: total_copy(k).start())
    own[2].wait()
    when(jnp.logical_not(outer), lambda: first_start((0, 2), (1, 1), (1, 3), (1, 2)))
    loads[3].wait()

    def gate_step(head, carry):
        lanes = by_head(head)
        gates[:, lanes] = silu(og_v[:, lanes].astype(jnp.float32)) * hgain_ref[...].astype(jnp.float32)
        return carry

    lax.fori_loop(0, heads, gate_step, 0)
    entry[...] = jnp.zeros_like(entry)
    for k in range(1, nz):
        when(jnp.logical_not(give_after(k)), lambda k=k: total_copy(k).wait_recv())
    for i in range(nz):
        origin = turn(i, nz)

        @pl.when(jnp.logical_and(origin != z, (origin < z) == (c == 0)))
        def _(origin=origin):
            factor, state = unpack(totals_in[origin])
            entry[...] = factor * entry[...] + state

    def enter_copy(w):
        return copy(made.at[w], enter.at[c, q], s3_out.at[w], s3_in.at[q], at(z, w, c))

    def enter_arrival(w):
        return copy(made.at[w], enter.at[c, w], s3_out.at[w], s3_in.at[w], at(z, w, c))

    def beside_copy(group):
        return copy(beside.at[group], enter.at[c, group], s4_out.at[group], s4_in.at[group], p_dev)

    def beside_arrival(group):
        return copy(beside.at[group], enter.at[1 - c, group], s4_out.at[group], s4_in.at[group], p_dev)

    for i in range(PLANE):
        origin = turn(i, PLANE)
        made[origin] = entry[...].astype(jnp.bfloat16)
        when(origin != q, lambda origin=origin: enter_copy(origin).start())
        factor, state = unpack(held[origin])
        entry[...] = factor * entry[...] + state
    enter[c, q] = made[q]
    when(outer, lambda: first_start((0, 2)))
    onward(0, 1)
    last(0, 0)
    spread(0, 2)
    for w in range(PLANE):
        when(w != q, lambda w=w: enter_arrival(w).wait_recv())
        factor, state = unpack(states[c, w])
        beside[w] = (factor * enter[c, w].astype(jnp.float32) + state).astype(jnp.bfloat16)
        beside_copy(w).start()
    for load in loads[4:]:
        load.wait()
    for w in range(PLANE):
        beside_arrival(w).wait_recv()

    when(outer, lambda: first_start((1, 2), (1, 3), (1, 1)))

    def mix_step(head, carry):
        lanes = by_head(head)
        group, i = head // per, lax.rem(head, per)
        mix = (
            locals_[:, lanes]
            + dot_nt(reach[0, :, lanes], enter[0, group, i])
            + dot_nt(reach[1, :, lanes], enter[1, group, i])
        )
        scale = lax.rsqrt(jnp.mean(mix * mix, axis=-1, keepdims=True) + NORM_EPS)
        mixed[:, lanes] = (mix * scale * gates[:, lanes]).astype(jnp.bfloat16)
        return carry

    lax.fori_loop(0, heads, mix_step, 0, unroll=4)
    chunk = columns // nz

    def hidden_step(i, carry):
        lanes = pl.ds(pl.multiple_of(i * chunk, chunk), chunk)
        part = dot_nn(mixed[...], wo_v[:, lanes]).astype(jnp.bfloat16).astype(jnp.float32)
        hidden = (res_v[:, lanes].astype(jnp.float32) + part).astype(jnp.bfloat16)
        res_v[:, lanes] = hidden
        hidden = hidden.astype(jnp.float32)
        return carry + jnp.sum(hidden * hidden, axis=-1, keepdims=True)

    squares = lax.fori_loop(0, columns // chunk, hidden_step, jnp.zeros((rows, 1), jnp.float32))
    scale = lax.rsqrt(squares / columns + NORM_EPS)
    for i in range(columns // width):
        lanes = pl.ds(i * width, width)
        gain = mgain_ref[i : i + 1].astype(jnp.float32)
        tok[z, :, lanes] = (res_v[:, lanes].astype(jnp.float32) * scale * gain).astype(jnp.bfloat16)

    def half(zz, h):
        return tok.at[zz, :, pl.ds(h * (columns // 2), columns // 2)]

    def up(zz, h):
        return copy(half(zz, h), half(zz, h), up_out.at[zz, h], up_in.at[zz, h], up_dev)

    def dn(zz, h):
        return copy(half(zz, h), half(zz, h), dn_out.at[zz, h], dn_in.at[zz, h], dn_dev)

    for h in (0, 1):
        when(z < nz - 1, lambda h=h: up(z, h).start())
        when(z > 0, lambda h=h: dn(z, h).start())

    def relay(k, h):
        @pl.when(z - k >= 0)
        def _():
            up(z - k, h).wait_recv()
            when(z < nz - 1, lambda: up(z - k, h).start())

        @pl.when(z + k < nz)
        def _():
            dn(z + k, h).wait_recv()
            when(z > 0, lambda: dn(z + k, h).start())

    def expand(zz):
        block = tok[zz]
        gate_act = dot_nn(block, w_v[0])
        up_act = dot_nn(block, w_v[1])
        inner[zz] = (silu(gate_act) * up_act).astype(jnp.bfloat16)

    def ordered(i):
        reach_dn, reach_up = z, nz - 1 - z
        near = jnp.minimum(reach_dn, reach_up)
        pair = (i + 1) // 2
        odd = lax.rem(i, 2)
        both = z + jnp.where(odd == 1, -pair, pair)
        single = jnp.where(reach_dn < reach_up, i, nz - 1 - i)
        return jnp.where(pair <= near, both, single)

    def lanes_of(s):
        return pl.ds(s * chunk, chunk)

    def lower(zz, s):
        out = dot_nt(inner[zz], w_v[2, s * chunk : (s + 1) * chunk])
        parts[zz, :, lanes_of(s)] = out.astype(jnp.bfloat16)

    def sum_up(zz, s):
        return copy(
            parts.at[zz, :, lanes_of(s)], terms.at[0, zz, :, lanes_of(s)], r_out.at[0], r_in.at[0, zz, s], up_dev
        )

    def sum_dn(zz, s):
        return copy(
            parts.at[zz, :, lanes_of(s)], terms.at[1, zz, :, lanes_of(s)], r_out.at[0], r_in.at[1, zz, s], dn_dev
        )

    def take(way, zz, s):
        (sum_up, sum_dn)[way](zz, s).wait_recv()
        parts[zz, :, lanes_of(s)] = (
            parts[zz, :, lanes_of(s)].astype(jnp.float32) + terms[way, zz, :, lanes_of(s)].astype(jnp.float32)
        ).astype(jnp.bfloat16)

    def ends(s, *far):
        for d in far:
            when(z == 0, lambda d=d: sum_up(d, s).start())
            when(z == nz - 1, lambda d=d: sum_dn(nz - 1 - d, s).start())

    def pass_up(at_z, zz, s):
        @pl.when(z == at_z)
        def _():
            take(0, zz, s)
            sum_up(zz, s).start()

    def pass_dn(at_z, zz, s):
        @pl.when(z == at_z)
        def _():
            take(1, zz, s)
            sum_dn(zz, s).start()

    def near_pass(s):
        pass_up(1, 2, s)
        pass_dn(2, 1, s)

    def far_pass(s):
        pass_up(1, 3, s)
        pass_dn(2, 0, s)

    def end_pass(s):
        pass_up(2, 3, s)
        pass_dn(1, 0, s)

    def work(lo, hi, act):
        def step(i, carry):
            act(ordered(i))
            return carry

        lax.fori_loop(lo, hi, step, 0)

    spread(0, 3)
    onward(0, 2)
    last(0, 1)
    onward(0, 3)
    spread(1, 0)
    spread(1, 1)
    relay(1, 0)
    last(0, 2)
    settle(0, 0)
    settle(0, 1)
    last(0, 3)
    onward(1, 0)
    spread(1, 2)
    relay(1, 1)
    settle(0, 2)
    settle(0, 3)
    work(1, 2, expand)
    onward(1, 1)
    spread(1, 3)
    relay(2, 0)
    last(1, 0)
    settle(1, 0)
    work(1, 2, lambda zz: lower(zz, 0))
    ends(0, 1)
    relay(2, 1)
    work(2, 3, expand)
    work(2, 3, lambda zz: lower(zz, 0))
    ends(0, 2)
    onward(1, 2)
    last(1, 1)
    settle(1, 1)
    work(1, 3, lambda zz: lower(zz, 1))
    ends(1, 2, 1)
    onward(1, 3)
    last(1, 2)
    settle(1, 2)
    near_pass(0)
    relay(3, 0)
    relay(3, 1)
    work(3, 4, expand)
    for s in range(3):
        work(3, 4, lambda zz, s=s: lower(zz, s))
        ends(s, 3)
    work(1, 3, lambda zz: lower(zz, 2))
    near_pass(1)
    last(1, 3)
    settle(1, 3)
    work(3, 4, lambda zz: lower(zz, 3))
    ends(3, 3)
    ends(2, 2, 1)
    work(1, 3, lambda zz: lower(zz, 3))
    ends(3, 2, 1)
    far_pass(0)
    far_pass(1)
    end_pass(0)
    far_pass(2)
    end_pass(1)
    work(0, 1, expand)
    for s in range(nz):
        work(0, 1, lambda zz, s=s: lower(zz, s))
    far_pass(3)
    end_pass(2)
    near_pass(2)
    end_pass(3)
    near_pass(3)

    def result(s):
        return pltpu.make_async_copy(mixed.at[:, lanes_of(s)], out_ref.at[:, lanes_of(s)], in_sem.at[6 + s])

    def finish(s):
        when(z > 0, lambda: sum_up(z, s).wait_recv())
        when(z < nz - 1, lambda: sum_dn(z, s).wait_recv())
        lanes = lanes_of(s)
        added = res_v[:, lanes].astype(jnp.float32) + parts[z, :, lanes].astype(jnp.float32)
        added = added + jnp.where(z > 0, terms[0, z, :, lanes].astype(jnp.float32), 0.0)
        added = added + jnp.where(z < nz - 1, terms[1, z, :, lanes].astype(jnp.float32), 0.0)
        mixed[:, lanes] = added.astype(jnp.bfloat16)
        result(s).start()

    for s in range(nz):
        finish(s)

    for s in range(nz):
        result(s).wait()
    def sent(src, sem, got_sem, there):
        copy(src, src, sem, got_sem, there).wait_send()

    sent(w_v.at[:, 0 : (nz - 1) * depth], w1_out.at[0], w1_in.at[0, 0], x_dev)
    sent(w_v.at[:, 0 : nz * depth], x_out.at[0], x_in.at[0, 0], x_dev)
    sent(w_v.at[:, 0 : nz * depth], y_out.at[0], y_in.at[0, 0], y_dev)
    sent(w_v.at[:, 0 : nz * depth], d_out.at[0], d_in.at[0, 0, 0], x_dev)
    sent(w_v.at[:, 0 : PLANE * nz * depth], p_out.at[0], p_in.at[0, 0, 0], p_dev)
    sent(parts.at[0 : nz - 1], r_out.at[0], r_in.at[0, 0, 0], x_dev)
    for k in range(1, nz):
        when(give_after(k), lambda k=k: total_copy(k).wait_send())
    for k in range(nz):
        for h in (0, 1):
            when(jnp.logical_and(z < nz - 1, k <= z), lambda k=k, h=h: up(k, h).wait_send())
            when(jnp.logical_and(z > 0, k >= z), lambda k=k, h=h: dn(k, h).wait_send())
    for w in range(PLANE):
        mate_copy(w).wait_send()
        beside_copy(w).wait_send()

        @pl.when(w != q)
        def _(w=w):
            chip_copy(w).wait_send()
            enter_copy(w).wait_send()


def layer(queries, forget_logits, values, gate_logits, slack, spike, head_gain, output_weight, residual, mixer_gain, gate, up, down):
    n = lax.axis_size("sp")
    nz = n // (PLANE * CORES)
    rows, columns = queries.shape
    heads, width = spike.shape[1], head_gain.shape[0]
    depth, units = gate.shape[0], gate.shape[1] // nz
    per = heads // PLANE
    bf16, f32 = jnp.bfloat16, jnp.float32
    anywhere = pl.BlockSpec(memory_space=pl.ANY)
    near = pl.BlockSpec(memory_space=pltpu.VMEM)
    dma = pltpu.SemaphoreType.DMA
    padded = width + PAD_ROWS

    def pairs(*shape):
        return [dma(shape), dma(shape)]

    def one_out(*shape):
        return [dma((1,)), dma(shape)]

    return pl.pallas_call(
        functools.partial(layer_kernel, nz),
        in_specs=[anywhere] * 5 + [near] * 4 + [anywhere] * 4,
        out_specs=anywhere,
        out_shape=jax.ShapeDtypeStruct((rows, columns), bf16),
        scratch_shapes=[
            pltpu.VMEM((rows, columns), bf16),
            pltpu.VMEM((2, rows, columns), bf16),
            pltpu.VMEM((rows, columns), bf16),
            pltpu.VMEM((rows, columns), bf16),
            pltpu.VMEM((rows, columns), bf16),
            pltpu.VMEM(output_weight.shape, bf16),
            pltpu.VMEM((3, n * depth, units), bf16),
            pltpu.VMEM((2, rows, columns), bf16),
            pltpu.VMEM((2, rows, columns), bf16),
            pltpu.VMEM((rows, columns), f32),
            pltpu.VMEM((rows, columns), f32),
            pltpu.VMEM((2, PLANE, per, padded, width), bf16),
            pltpu.VMEM((PLANE, per, padded, width), bf16),
            pltpu.VMEM((PLANE, per, padded, width), bf16),
            pltpu.VMEM((PLANE, per, padded, width), bf16),
            pltpu.VMEM((per, padded, width), bf16),
            pltpu.VMEM((nz, per, padded, width), bf16),
            pltpu.VMEM((per, width, width), f32),
            pltpu.VMEM((PLANE, per, width, width), bf16),
            pltpu.VMEM((2, PLANE, per, width, width), bf16),
            pltpu.VMEM((PLANE, per, width, width), bf16),
            pltpu.VMEM((rows, columns), bf16),
            pltpu.VMEM((nz, rows, columns), bf16),
            pltpu.VMEM((nz, rows, units), bf16),
            pltpu.VMEM((nz, rows, columns), bf16),
            pltpu.VMEM((2, nz, rows, columns), bf16),
            dma((6 + nz,)),
            dma((3,)),
            *one_out(3, nz),
            *one_out(2, nz),
            *one_out(2, nz),
            *one_out(2, 2, nz),
            *one_out(2, nz, PLANE),
            *pairs(PLANE),
            *pairs(PLANE),
            *pairs(nz),
            *pairs(PLANE),
            *pairs(PLANE),
            *pairs(nz, 2),
            *pairs(nz, 2),
            *one_out(2, nz, nz),
        ],
        compiler_params=pltpu.CompilerParams(
            collective_id=7, has_side_effects=True, vmem_limit_bytes=60 * 1024 * 1024
        ),
        name="layer",
    )(
        queries, forget_logits, values, gate_logits, residual, slack.reshape(1, columns), spike.T,
        head_gain.reshape(1, width), mixer_gain.reshape(columns // width, width), output_weight, gate, up, down.T,
    )


def local(
    queries,
    forget_logits,
    value_matrix,
    output_gate_logits,
    forget_slack,
    spike_log_forget,
    head_norm_gain,
    output_weight,
    residual,
    mixer_norm_gain,
    mixer_gate_weight,
    mixer_up_weight,
    mixer_down_weight,
):
    n, tp = lax.axis_size("sp"), lax.axis_size("tp")
    nz, tail = n // (PLANE * CORES), n % (PLANE * CORES)
    if tp == 1 and tail == 0 and nz == PLANE and mixer_gate_weight.shape[1] % (128 * nz) == 0:
        return layer(
            queries,
            forget_logits,
            value_matrix,
            output_gate_logits,
            forget_slack,
            spike_log_forget,
            head_norm_gain,
            output_weight,
            residual,
            mixer_norm_gain,
            mixer_gate_weight,
            mixer_up_weight,
            mixer_down_weight,
        )
    g = GROUP
    row_count = queries.shape[0]
    depth, units = mixer_gate_weight.shape
    far = [[b * g + j for b in range(n // g)] for j in range(g)]

    def cut(weight):
        return weight.reshape(depth, g, units // g).transpose(1, 0, 2)

    pieces = reshard([cut(mixer_gate_weight), cut(mixer_up_weight), cut(mixer_down_weight.T)], g, 2)
    gate_weight, up_weight, down_weight = (
        lax.all_gather(
            p.reshape(g * depth, units // g), "sp", axis=0, tiled=True, axis_index_groups=far
        )
        for p in pieces
    )

    local_out, reach, states = sweep(
        queries, forget_logits, value_matrix, forget_slack, spike_log_forget
    )
    entered = exchange(states)
    part = project(local_out, reach, entered, head_norm_gain, output_gate_logits, output_weight)
    part_rows = row_count // tp
    if tp > 1:
        part = lax.psum_scatter(part, "tp", scatter_dimension=0, tiled=True)
        residual = lax.dynamic_slice_in_dim(
            residual, lax.axis_index("tp") * part_rows, part_rows, 0
        )
    hidden = (residual.astype(jnp.float32) + part.astype(jnp.float32)).astype(jnp.bfloat16)
    hidden_f = hidden.astype(jnp.float32)
    normed = (
        hidden_f
        * lax.rsqrt(jnp.mean(hidden_f * hidden_f, axis=-1, keepdims=True) + NORM_EPS)
        * mixer_norm_gain.astype(jnp.float32)
    ).astype(jnp.bfloat16)
    normed = gather(normed, g, 4)
    if tp > 1:
        normed = lax.all_gather(normed, "tp", axis=0, tiled=True)
    gate_act = dot_nn(normed, gate_weight)
    up_act = dot_nn(normed, up_weight)
    inner = (silu(gate_act) * up_act).astype(jnp.bfloat16)
    lowered = dot_nt(inner, down_weight).astype(jnp.bfloat16)
    if tp > 1:
        lowered = lax.psum_scatter(lowered, "tp", scatter_dimension=0, tiled=True)
    (terms,) = reshard([lowered.reshape(g, part_rows, lowered.shape[1])], g, 3)
    added = jnp.sum(terms.astype(jnp.float32), axis=0)
    return (hidden_f + added).astype(jnp.bfloat16)


def solution(mesh):
    placed = (
        P("sp", "tp"),
        P(None, "sp", "tp"),
        P("sp", "tp"),
        P("sp", "tp"),
        P("tp"),
        P("sp", "tp"),
        P(),
        P("tp", None),
        P("sp", None),
        P(),
        P("sp", "tp"),
        P("sp", "tp"),
        P("tp", "sp"),
    )
    return jax.shard_map(
        local, mesh=mesh, in_specs=placed, out_specs=P(("sp", "tp"), None), check_vma=False
    )
```
